128 devices in a mesh: dp: 4 (over x), kv: 16 (over z, y), tp: 2 (over core).
Axes of the slice: x: 4, y: 4, z: 4, core: 2. Of those that a mesh axis runs over, the one named last changes fastest.
Arguments:
- tokens: bfloat16 [8192, 2048], P('dp', 'kv'), may hold values from -70 to 70
- pre_gain: float32 [2048], replicated, may hold values from 0.1 to 1.9
- query_weight: bfloat16 [2048, 1024], P(None, 'tp'), may hold values from -0.125 to 0.125
- key_weight: bfloat16 [2048, 1024], P(None, 'tp'), may hold values from -0.125 to 0.125
- value_weight: bfloat16 [2048, 1024], P(None, 'tp'), may hold values from -0.125 to 0.125
- gate_weight: bfloat16 [2048, 1024], P(None, 'tp'), may hold values from -0.125 to 0.125
- beta_weight: bfloat16 [2048, 8], replicated, may hold values from -0.125 to 0.125
- decay_weight: bfloat16 [2048, 8], replicated, may hold values from -0.125 to 0.125
- decay_log: float32 [8], P('tp'), may hold values from -3 to 0.5
- head_gain: float32 [128], replicated, may hold values from 0.1 to 1.9
- out_weight: bfloat16 [1024, 2048], P('tp', 'kv'), may hold values from -1 to 1
- post_gain: float32 [2048], P(('kv', 'tp')), may hold values from 0.1 to 1.9
- saved_state: float32 [2048, 8, 128, 128], P(('dp', 'kv'), 'tp'), may hold values from -4 to 4
- earlier_keys: bfloat16 [2048, 4, 8, 128], P(('dp', 'kv'), None, 'tp'), may hold values from -6 to 6
- earlier_values: bfloat16 [2048, 4, 8, 128], P(('dp', 'kv'), None, 'tp'), may hold values from -6 to 6
- earlier_rates: float32 [2048, 4, 8], P(('dp', 'kv'), None, 'tp'), may hold values from 0.05 to 0.95
- earlier_decays: float32 [2048, 4, 8], P(('dp', 'kv'), None, 'tp'), may hold values from -1.5 to -0.02
- accepted: int32 [2048], P(('dp', 'kv')), may hold values from 0 to 4
Outputs:
- mixed: bfloat16 [8192, 2048], P('dp', ('kv', 'tp'))
- committed: float32 [2048, 8, 128, 128], P(('dp', 'kv'), 'tp')
The draws below stay inside these ranges and needn't reach their ends.
All inputs are finite; a program needn't handle non-finite values.
Results may differ from the reference program's by a relative error of at most 0.011.
Values may be sent and summed in bfloat16 or wider, within the bound.
A program may use at most 128 MiB of HBM per device.

```python
import jax
import jax.numpy as jnp
from jax import lax

D = 2048
HEADS = 8
HEAD = 128
PROPOSALS = 4
SEQS = 2048
ROWS = 8192


def draw_tokens(key, part):
    columns = jnp.arange(D, dtype=jnp.float32)
    rising = 1.0 + 3.0 * columns / D
    base = jnp.clip(jax.random.normal(key, (ROWS, D), jnp.float32), -5.0, 5.0)
    return (base * rising).astype(jnp.bfloat16)


def draw_out_weight(key, part):
    columns = jnp.arange(D, dtype=jnp.float32)
    rising = (1.0 + 3.0 * columns / D) * (HEADS * HEAD) ** (-0.5)
    base = jnp.clip(jax.random.normal(key, (HEADS * HEAD, D), jnp.float32), -6.0, 6.0)
    return jnp.clip(base * rising, -1.0, 1.0).astype(jnp.bfloat16)


def place_ends(entries, stream_key, smallest, top_value):
    dims = entries.shape
    spot = [jax.random.randint(jax.random.fold_in(stream_key, axis), (), 0, dims[axis]) for axis in range(len(dims))]
    entries = entries.at[tuple(spot)].set(smallest)
    longest = dims.index(max(dims))
    spot[longest] = (spot[longest] + 1) % dims[longest]
    return entries.at[tuple(spot)].set(top_value)


def level_of(key, extent, cuts, least, high):
    def one(dim, shards_of):
        heights = jax.random.uniform(jax.random.fold_in(jax.random.fold_in(key, 6), dim), (shards_of,), jnp.float32, least / len(cuts), high / len(cuts))
        return jnp.repeat(jnp.exp(heights), extent[dim] // shards_of).reshape((-1,) + (1,) * (len(extent) - dim - 1))

    loudness = one(*cuts[0])
    for cut in cuts[1:]:
        loudness = loudness * one(*cut)
    return loudness


def normal_values(rng, extent, deviation, most, cuts=(), kind=jnp.bfloat16):
    values = deviation * jax.random.normal(rng, extent, jnp.float32)
    if cuts:
        values = values * level_of(rng, extent, cuts, -0.22, 0.18)
    return jnp.clip(values, -most, most).astype(kind)


def setup_inputs(seed: int = 0) -> dict:
    splits = jax.random.split(jax.random.key(seed), 19)
    return {
        "tokens": draw_tokens(jax.random.fold_in(splits[18], 71), 0),
        "pre_gain": jnp.clip(1.0 + 0.18 * jax.random.normal(splits[1], (D,), jnp.float32), 0.1, 1.9),
        "query_weight": normal_values(splits[2], (D, HEADS * HEAD), D ** -0.5, 0.125, ((1, 2),)),
        "key_weight": normal_values(splits[3], (D, HEADS * HEAD), D ** -0.5, 0.125, ((1, 2),)),
        "value_weight": normal_values(splits[4], (D, HEADS * HEAD), D ** -0.5, 0.125, ((1, 2),)),
        "gate_weight": normal_values(splits[5], (D, HEADS * HEAD), D ** -0.5, 0.125, ((1, 2),)),
        "beta_weight": normal_values(splits[6], (D, HEADS), D ** -0.5, 0.125),
        "decay_weight": normal_values(splits[7], (D, HEADS), D ** -0.5, 0.125),
        "decay_log": jnp.clip(-3.0 + 3.5 * jax.random.uniform(splits[8], (HEADS,), jnp.float32) ** level_of(splits[8], (HEADS,), ((0, 2),), -0.2, 0.2), -3.0, 0.5),
        "head_gain": jnp.clip(1.0 + 0.18 * jax.random.normal(splits[9], (HEAD,), jnp.float32), 0.1, 1.9),
        "out_weight": draw_out_weight(jax.random.fold_in(splits[18], 71), 0),
        "post_gain": jnp.clip(1.0 + 0.18 * jax.random.normal(splits[11], (D,), jnp.float32), 0.1, 1.9),
        "saved_state": normal_values(splits[12], (SEQS, HEADS, HEAD, HEAD), 0.3, 4.0, ((0, 64), (1, 2)), jnp.float32),
        "earlier_keys": normal_values(splits[13], (SEQS, PROPOSALS, HEADS, HEAD), 1.0, 6.0, ((0, 64), (2, 2))),
        "earlier_values": normal_values(splits[14], (SEQS, PROPOSALS, HEADS, HEAD), 1.0, 6.0, ((0, 64), (2, 2))),
        "earlier_rates": jnp.clip(0.05 + 0.9 * jax.random.uniform(splits[15], (SEQS, PROPOSALS, HEADS), jnp.float32) ** level_of(splits[15], (SEQS, PROPOSALS, HEADS), ((0, 64), (2, 2)), -0.2, 0.2), 0.05, 0.95),
        "earlier_decays": jnp.clip(-1.5 + 1.48 * jax.random.uniform(splits[16], (SEQS, PROPOSALS, HEADS), jnp.float32) ** level_of(splits[16], (SEQS, PROPOSALS, HEADS), ((0, 64), (2, 2)), -0.2, 0.2), -1.5, -0.02),
        "accepted": place_ends(jax.random.randint(splits[17], (SEQS,), 0, PROPOSALS + 1), jax.random.fold_in(splits[17], 1), 0, PROPOSALS).astype(jnp.int32),
    }


def unit_norm(values):
    return values * lax.rsqrt(lax.optimization_barrier(jnp.sum(values * values, axis=-1, keepdims=True)) + 1e-06)

def advance(current, key_row, value_row, rate_now, log_decay):
    recalled = lax.optimization_barrier(jnp.sum(key_row[..., :, None] * current, axis=-2))
    rate_cube = rate_now[..., None, None]
    current = current - rate_cube * key_row[..., :, None] * recalled[..., None, :]
    return jnp.exp(log_decay)[..., None, None] * current + rate_cube * key_row[..., :, None] * value_row[..., None, :]

def run_heads(saved_state, earlier_keys, earlier_values, earlier_rates, earlier_decays, accepted, queries, keys_unit, values_act, rates, decays):
    current = saved_state
    proposals = earlier_keys.shape[1]
    for position in range(proposals):
        live = (position < accepted).astype(jnp.float32)
        live = live.reshape(live.shape + (1,) * (earlier_rates.ndim - 2))
        current = advance(current, earlier_keys[:, position], earlier_values[:, position], earlier_rates[:, position] * live, earlier_decays[:, position] * live)
    committed = current
    outputs = []
    for position in range(proposals):
        current = advance(current, keys_unit[:, position], values_act[:, position], rates[:, position], decays[:, position])
        outputs.append(lax.optimization_barrier(jnp.sum(queries[:, position][..., :, None] * current, axis=-2)))
    return (committed, jnp.stack(outputs, axis=1))

def reference(tokens, pre_gain, query_weight, key_weight, value_weight, gate_weight, beta_weight, decay_weight, decay_log, head_gain, out_weight, post_gain, saved_state, earlier_keys, earlier_values, earlier_rates, earlier_decays, accepted):
    widened = tokens.astype(jnp.float32)
    inverse = lax.rsqrt(lax.optimization_barrier(jnp.mean(widened * widened, axis=1, keepdims=True)) + 1e-06)
    scaled = (widened * pre_gain).astype(jnp.bfloat16)

    def project(weight):
        return jnp.dot(scaled, weight, preferred_element_type=jnp.float32) * inverse

    def heads_of(values):
        return values.reshape(SEQS, PROPOSALS, HEADS, HEAD)
    queries = unit_norm(jax.nn.silu(heads_of(project(query_weight)))) * HEAD ** (-0.5)
    keys_unit = unit_norm(jax.nn.silu(heads_of(project(key_weight))))
    values_act = jax.nn.silu(heads_of(project(value_weight)))
    gates_raw = heads_of(project(gate_weight))
    rates = jax.nn.sigmoid(project(beta_weight)).reshape(SEQS, PROPOSALS, HEADS)
    decays = -jnp.exp(decay_log) * jax.nn.softplus(project(decay_weight)).reshape(SEQS, PROPOSALS, HEADS)
    earlier_unit = unit_norm(earlier_keys.astype(jnp.float32))
    earlier_vals = earlier_values.astype(jnp.float32)

    def per_head(items):
        return run_heads(items[0], items[1], items[2], items[3], items[4], accepted, items[5], items[6], items[7], items[8], items[9])
    items = (jnp.moveaxis(saved_state, 1, 0), jnp.moveaxis(earlier_unit, 2, 0), jnp.moveaxis(earlier_vals, 2, 0), jnp.moveaxis(earlier_rates, 2, 0), jnp.moveaxis(earlier_decays, 2, 0), jnp.moveaxis(queries, 2, 0), jnp.moveaxis(keys_unit, 2, 0), jnp.moveaxis(values_act, 2, 0), jnp.moveaxis(rates, 2, 0), jnp.moveaxis(decays, 2, 0))
    committed, reads = lax.map(per_head, items)
    committed = jnp.moveaxis(committed, 0, 1)
    reads = jnp.moveaxis(reads, 0, 2)
    normed = reads * lax.rsqrt(lax.optimization_barrier(jnp.mean(reads * reads, axis=-1, keepdims=True)) + 1e-06) * head_gain
    attended = (normed * jax.nn.silu(gates_raw)).reshape(ROWS, HEADS * HEAD).astype(jnp.bfloat16)
    projected = jnp.dot(attended, out_weight, preferred_element_type=jnp.float32)
    factor = lax.rsqrt(lax.optimization_barrier(jnp.mean(projected * projected, axis=1, keepdims=True)) + 1e-06)
    mixed = (projected * factor * post_gain).astype(jnp.bfloat16)
    return (mixed, committed)
```

```python
import functools

import jax
import jax.numpy as jnp
from jax import lax
from jax.experimental import pallas as pl
from jax.experimental.pallas import tpu as pltpu
from jax.sharding import PartitionSpec as P

MESH = pl.DeviceIdType.MESH
F32 = jnp.float32
BF16 = jnp.bfloat16
HIGH = lax.Precision.HIGHEST
VM = pltpu.VMEM
NT = (((1,), (1,)), ((), ()))
TN = (((0,), (0,)), ((), ()))


def mm(a, b):
    return jnp.dot(a, b, preferred_element_type=F32)


def mm_nt(a, b):
    return lax.dot_general(a, b, NT, preferred_element_type=F32)


def silu(v):
    return v / (1.0 + jnp.exp(-v))


def unit(v):
    return v * lax.rsqrt(jnp.sum(v * v, axis=-1, keepdims=True) + 1e-06)


def quad_rows(wide, rows):
    own = lax.broadcasted_iota(jnp.int32, (rows, 128), 0) % 16 // 4
    out = wide[:, 0:128]
    for q in range(1, 4):
        out = jnp.where(own == q, wide[:, 128 * q : 128 * q + 128], out)
    return out


def masks():
    r = lax.broadcasted_iota(jnp.int32, (128, 128), 0)
    c = lax.broadcasted_iota(jnp.int32, (128, 128), 1)
    same = r // 4 == c // 4
    return r == c, same & (c < r), same & (c <= r)


def as_row(col, eye):
    return jnp.sum(jnp.where(eye, col, 0.0), axis=0, keepdims=True)


def ratios(c_col, c_row, keep):
    return jnp.where(keep, jnp.exp(jnp.where(keep, c_col - c_row, 0.0)), 0.0)


def nilpotent(a):
    ab = a.astype(BF16)
    square = mm(ab, ab)
    return square - a - mm(ab, square.astype(BF16))


def main_kernel(
    n,
    tokens, pre_gain, wq, wk, wv, wg, beta_t, decay_t, decay_log, head_gain, out_w, saved,
    ekeys, evals, erates, edecays, accepted,
    state, mixed_in,
    tok, x, w, ow, wt, state_b, ek, ev, k1b, r1, rq, k2b, q2b, v2, gates, tot, proj, scal, ssq, att,
    part, psend, precv, msend,
    tok_sem, ow_sem, s_sem, w_sem, tsend, trecv, gsend, grecv, xsend, xrecv, osend, orecv,
):
    me = lax.axis_index("kv")
    core = lax.axis_index("tp")
    width = n * 128

    load_tok = pltpu.make_async_copy(tokens, tok, tok_sem)
    load_ow = pltpu.make_async_copy(out_w, ow, ow_sem)
    load_tok.start()
    load_ow.start()
    load_s = [pltpu.make_async_copy(saved.at[pl.ds(4 * t, 4)], state.at[pl.ds(4 * t, 4)], s_sem.at[t]) for t in range(8)]
    for c in load_s:
        c.start()
    load_w = [pltpu.make_async_copy(src, w.at[i], w_sem.at[i]) for i, src in enumerate((wq, wk, wv, wg))]
    for c in load_w:
        c.start()

    barrier = pltpu.get_barrier_semaphore()
    for d in range(1, n):
        pl.semaphore_signal(barrier, inc=1, device_id={"kv": lax.rem(me + d, n), "tp": core}, device_id_type=MESH)
    pl.semaphore_signal(barrier, inc=1, device_id={"kv": me, "tp": 1 - core}, device_id_type=MESH)

    eye, strict, incl = masks()
    load_ow.wait()
    wt[pl.ds(me, 1)] = mm_nt(jnp.where(eye, 1.0, 0.0).astype(BF16), ow[...]).astype(BF16)[None]
    load_tok.wait()
    x[pl.ds(me, 1)] = tok[pl.ds(pl.multiple_of(me * 128, 128), 128), :][None]

    pl.semaphore_wait(barrier, n)

    def to_peer(src, dst, ssem, rsem, peer):
        return pltpu.make_async_remote_copy(
            src_ref=src, dst_ref=dst, send_sem=ssem, recv_sem=rsem,
            device_id={"kv": peer, "tp": core}, device_id_type=MESH,
        )

    def send_tok(d):
        peer = lax.rem(me + d, n)
        rows = pl.ds(pl.multiple_of(peer * 128, 128), 128)
        return to_peer(tok.at[rows, :], x.at[me], tsend.at[d], trecv.at[me], peer)

    def send_wt(d):
        peer = lax.rem(me + d, n)
        return to_peer(wt.at[me], wt.at[me], gsend.at[d], grecv.at[me], peer)

    for d in range(1, n):
        send_tok(d).start()
    for d in range(1, n):
        send_wt(d).start()

    keys = unit(ekeys[...].astype(F32))
    ek[...] = keys
    ev[...] = evals[...].astype(F32)
    count = accepted[...]
    total = jnp.zeros((4, 32), F32)
    rate_p, cum_p = [], []
    for p in range(4):
        live = jnp.where(p < count, 1.0, 0.0)
        total = total + edecays[p] * live
        rate_p.append(erates[p] * live)
        cum_p.append(total)
    row = lax.broadcasted_iota(jnp.int32, (128, 32), 0)
    seq = lax.broadcasted_iota(jnp.int32, (128, 32), 1)

    def expand(pieces):
        out = jnp.zeros((128, 4), F32)
        for p in range(4):
            pick = jnp.where(row == 4 * seq + p, 1.0, 0.0)
            out = out + lax.dot_general(pick, pieces[p], NT, precision=HIGH, preferred_element_type=F32)
        return out

    rate1 = expand(rate_p)
    cum1 = expand(cum_p)
    tot1 = expand([total] * 4)
    for h in range(4):
        k1b[h] = ek[pl.ds(h, 128, stride=4), :].astype(BF16)
        tot[h] = jnp.broadcast_to(jnp.exp(tot1[:, h : h + 1]), (128, 128))
    for c in load_s:
        c.wait()

    def recall(t, _):
        rows = pl.ds(pl.multiple_of(16 * t, 16), 16)
        for h in range(4):
            wide = jnp.concatenate([state[4 * t + q, h].astype(BF16) for q in range(4)], axis=1)
            r1[h, rows, :] = quad_rows(mm(k1b[h, rows, :], wide), 16)
        return 0

    lax.fori_loop(0, 8, recall, 0)

    for h in range(4):
        b = rate1[:, h : h + 1]
        c_col = cum1[:, h : h + 1]
        kb = k1b[h]
        a = b * ratios(c_col, as_row(c_col, eye), strict) * mm_nt(kb, kb)
        rhs = b * (ev[pl.ds(h, 128, stride=4), :] - jnp.exp(c_col) * r1[h])
        u = rhs + mm(nilpotent(a).astype(BF16), rhs.astype(BF16))
        r1[h] = u * jnp.exp(tot1[:, h : h + 1] - c_col)

    own = lax.broadcasted_iota(jnp.int32, (16, 128), 0) // 4

    def fold(t, _):
        rows = pl.ds(pl.multiple_of(16 * t, 16), 16)
        for h in range(4):
            u = r1[h, rows, :]
            wide = jnp.concatenate([jnp.where(own == q, u, 0.0) for q in range(4)], axis=1).astype(BF16)
            step = lax.dot_general(k1b[h, rows, :], wide, TN, preferred_element_type=F32)
            for q in range(4):
                new = state[4 * t + q, h] * tot[h, pl.ds(16 * t + 4 * q, 1), :] + step[:, 128 * q : 128 * q + 128]
                state[4 * t + q, h] = new
                state_b[h, t, :, 128 * q : 128 * q + 128] = new.astype(BF16)
        return 0

    lax.fori_loop(0, 8, fold, 0)

    for c in load_w:
        c.wait()
    proj[...] = jnp.zeros_like(proj)
    scal[...] = jnp.zeros_like(scal)
    ssq[...] = jnp.zeros_like(ssq)
    for g in range(n // 4):
        group = lax.rem(me // 4 + g, n // 4)
        for i in range(4):
            src = 4 * group + i

            @pl.when(src != me)
            def _():
                to_peer(tok.at[pl.ds(0, 128), :], x.at[src], tsend.at[0], trecv.at[src], src).wait_recv()

        pieces = []
        square = jnp.zeros((128, 128), F32)
        for i in range(4):
            wide = x[pl.ds(4 * group + i, 1)][0].astype(F32)
            square = square + wide * wide
            pieces.append((wide * pre_gain[pl.ds(4 * group + i, 1), :]).astype(BF16))
        scaled = jnp.concatenate(pieces, axis=1)
        ssq[...] += square
        cols = pl.ds(pl.multiple_of(group * 512, 512), 512)
        scal[0] += mm_nt(scaled, beta_t[:, cols])
        scal[1] += mm_nt(scaled, decay_t[:, cols])
        for i in range(4):
            proj[i] += mm(scaled, w[i, cols, :])
    inverse = lax.rsqrt(jnp.sum(ssq[...], axis=1, keepdims=True) / width + 1e-06)
    beta_raw = scal[0] * inverse
    decay_raw = scal[1] * inverse
    rates8 = 1.0 / (1.0 + jnp.exp(-beta_raw))
    soft8 = jnp.maximum(decay_raw, 0.0) + jnp.log1p(jnp.exp(-jnp.abs(decay_raw)))
    for h in range(4):
        lanes = slice(128 * h, 128 * h + 128)
        q2b[h] = (unit(silu(proj[0, :, lanes] * inverse)) * 128 ** (-0.5)).astype(BF16)
        k2b[h] = unit(silu(proj[1, :, lanes] * inverse)).astype(BF16)
        v2[h] = silu(proj[2, :, lanes] * inverse)
        gates[h] = silu(proj[3, :, lanes] * inverse) * head_gain[...]

    def recall_new(t, _):
        rows = pl.ds(pl.multiple_of(16 * t, 16), 16)
        for h in range(4):
            both = jnp.concatenate([k2b[h, rows, :], q2b[h, rows, :]], axis=0)
            out = quad_rows(mm(both, state_b[h, t]), 32)
            r1[h, rows, :] = out[:16]
            rq[h, rows, :] = out[16:]
        return 0

    lax.fori_loop(0, 8, recall_new, 0)

    upper = core > 0
    pos = lax.broadcasted_iota(jnp.int32, (128, 1), 0) % 4
    for h in range(4):
        b = jnp.where(upper, rates8[:, h + 4 : h + 5], rates8[:, h : h + 1])
        g = jnp.where(upper, soft8[:, h + 4 : h + 5], soft8[:, h : h + 1])
        g = -jnp.exp(jnp.full((1, 1), decay_log[0, h], F32)) * g
        c_col = jnp.sum(jnp.where(incl, as_row(g, eye), 0.0), axis=1, keepdims=True)
        ratio = ratios(c_col, as_row(c_col, eye), incl)
        kb = k2b[h]
        a = jnp.where(strict, b * ratio * mm_nt(kb, kb), 0.0)
        seen = ratio * mm_nt(q2b[h], kb)
        seen = seen + mm(seen.astype(BF16), nilpotent(a).astype(BF16))
        grown = jnp.exp(c_col)
        rhs = b * (v2[h] - grown * r1[h])
        reads = grown * rq[h] + mm(seen.astype(BF16), rhs.astype(BF16))
        normed = reads * lax.rsqrt(jnp.mean(reads * reads, axis=-1, keepdims=True) + 1e-06)
        att[:, 128 * h : 128 * h + 128] = (normed * gates[h]).astype(BF16)

    for d in range(1, n):
        src = lax.rem(me + d, n)
        to_peer(wt.at[me], wt.at[src], gsend.at[0], grecv.at[src], src).wait_recv()
    per = n // 4

    def swap(c):
        rows = pl.ds(c * per, per)
        return pltpu.make_async_remote_copy(
            src_ref=psend.at[rows], dst_ref=precv.at[rows], send_sem=xsend.at[c], recv_sem=xrecv.at[c],
            device_id={"kv": me, "tp": 1 - core}, device_id_type=MESH,
        )

    attended = att[...]
    for c in range(4):
        for i in range(c * per, c * per + per):
            out = mm_nt(wt[i], attended)
            part[i] = out
            psend[i] = out.astype(BF16)
        swap(c).start()
    squares = jnp.zeros((128, 128), F32)
    for c in range(4):
        swap(c).wait_recv()
        for i in range(c * per, c * per + per):
            both = part[i] + precv[i].astype(F32)
            squares = squares + both * both
    factor = lax.rsqrt(jnp.sum(squares, axis=0, keepdims=True) / width + 1e-06)
    half = pl.ds(pl.multiple_of(core * 64, 64), 64)
    for i in range(n):
        both = part[i, half, :] + precv[i, half, :].astype(F32)
        msend[i] = (both * factor).astype(BF16)
    mixed_in[pl.ds(me, 1)] = msend[pl.ds(me, 1)]

    def send_out(d):
        peer = lax.rem(me + d, n)
        return to_peer(msend.at[peer], mixed_in.at[me], osend.at[d], orecv.at[me], peer)

    for d in range(1, n):
        send_out(d).start()
    for d in range(1, n):
        src = lax.rem(me + d, n)
        to_peer(msend.at[me], mixed_in.at[src], osend.at[0], orecv.at[src], src).wait_recv()
    for d in range(1, n):
        send_tok(d).wait_send()
        send_wt(d).wait_send()
        send_out(d).wait_send()
    for c in range(4):
        swap(c).wait_send()


def last_kernel(n, state, mixed_in, post_gain, committed, mixed, sem):
    copies = [pltpu.make_async_copy(state.at[pl.ds(8 * t, 8)], committed.at[pl.ds(8 * t, 8)], sem.at[t]) for t in range(4)]
    for c in copies:
        c.start()
    i = lax.broadcasted_iota(jnp.int32, (64, 64), 0)
    j = lax.broadcasted_iota(jnp.int32, (64, 64), 1)
    gain = jnp.sum(jnp.where(i == j, post_gain[...], 0.0), axis=1, keepdims=True)
    for k in range(n):
        mixed[:, 128 * k : 128 * k + 128] = (mixed_in[k].astype(F32) * gain).astype(BF16)
    for c in copies:
        c.wait()


def local(
    n,
    tokens, pre_gain, query_weight, key_weight, value_weight, gate_weight, beta_weight, decay_weight, decay_log,
    head_gain, out_weight, post_gain, saved_state, earlier_keys, earlier_values, earlier_rates, earlier_decays, accepted,
):
    any_spec = pl.BlockSpec(memory_space=pl.ANY)
    vmem = pl.BlockSpec(memory_space=VM)
    smem = pl.BlockSpec(memory_space=pltpu.SMEM)
    dma = pltpu.SemaphoreType.DMA
    heads = (4, 128, 128)
    state, mixed_in = pl.pallas_call(
        functools.partial(main_kernel, n),
        out_shape=(VM(saved_state.shape, F32), VM((n, 64, 128), BF16)),
        in_specs=[any_spec, vmem, any_spec, any_spec, any_spec, any_spec, vmem, vmem, smem, vmem, any_spec, any_spec]
        + [vmem] * 5,
        out_specs=(vmem, vmem),
        scratch_shapes=[
            VM((n * 128, 128), BF16),
            VM((n, 128, 128), BF16),
            VM((4, n * 128, 512), BF16),
            VM((512, 128), BF16),
            VM((n, 128, 512), BF16),
            VM((4, 8, 128, 512), BF16),
            VM((512, 128), F32),
            VM((512, 128), F32),
            VM(heads, BF16),
            VM(heads, F32),
            VM(heads, F32),
            VM(heads, BF16),
            VM(heads, BF16),
            VM(heads, F32),
            VM(heads, F32),
            VM(heads, F32),
            VM((4, 128, 512), F32),
            VM((2, 128, 8), F32),
            VM((128, 128), F32),
            VM((128, 512), BF16),
            VM((n, 128, 128), F32),
            VM((n, 128, 128), BF16),
            VM((n, 128, 128), BF16),
            VM((n, 64, 128), BF16),
            dma, dma, dma((8,)), dma((4,)), dma((n,)), dma((n,)), dma((n,)), dma((n,)), dma((4,)), dma((4,)), dma((n,)), dma((n,)),
        ],
        compiler_params=pltpu.CompilerParams(collective_id=0, has_side_effects=True, vmem_limit_bytes=48 << 20),
        name="delta_step",
    )(
        tokens, pre_gain.reshape(n, 128), query_weight, key_weight, value_weight, gate_weight, beta_weight.T,
        decay_weight.T, decay_log.reshape(1, 4), head_gain.reshape(1, 128), out_weight, saved_state,
        earlier_keys.reshape(512, 128), earlier_values.reshape(512, 128), earlier_rates.transpose(1, 2, 0),
        earlier_decays.transpose(1, 2, 0), accepted.reshape(1, 32),
    )
    committed, mixed = pl.pallas_call(
        functools.partial(last_kernel, n),
        out_shape=(jax.ShapeDtypeStruct(saved_state.shape, F32), jax.ShapeDtypeStruct((64, n * 128), BF16)),
        in_specs=[vmem] * 3,
        out_specs=(any_spec, vmem),
        scratch_shapes=[dma((4,))],
        compiler_params=pltpu.CompilerParams(vmem_limit_bytes=16 << 20),
        name="write_out",
    )(state, mixed_in, post_gain.reshape(1, 64))
    return mixed.T, committed


def solution(mesh):
    placed = (
        P("dp", "kv"), P(), P(None, "tp"), P(None, "tp"), P(None, "tp"), P(None, "tp"), P(), P(), P("tp"), P(),
        P("tp", "kv"), P(("kv", "tp")), P(("dp", "kv"), "tp", None, None), P(("dp", "kv"), None, "tp", None),
        P(("dp", "kv"), None, "tp", None), P(("dp", "kv"), None, "tp"), P(("dp", "kv"), None, "tp"), P(("dp", "kv")),
    )
    return jax.shard_map(
        functools.partial(local, mesh.shape["kv"]),
        mesh=mesh,
        in_specs=placed,
        out_specs=(P("dp", ("kv", "tp")), P(("dp", "kv"), "tp", None, None)),
        check_vma=False,
    )
```

```python
import functools

import jax
import jax.numpy as jnp
from jax import lax
from jax.experimental import pallas as pl
from jax.experimental.pallas import tpu as pltpu
from jax.sharding import PartitionSpec as P

MESH = pl.DeviceIdType.MESH
F32 = jnp.float32
BF16 = jnp.bfloat16
HIGH = lax.Precision.HIGHEST
VM = pltpu.VMEM
NT = (((1,), (1,)), ((), ()))
TN = (((0,), (0,)), ((), ()))


def mm(a, b):
    return jnp.dot(a, b, preferred_element_type=F32)


def mm_nt(a, b):
    return lax.dot_general(a, b, NT, preferred_element_type=F32)


def silu(v):
    return v / (1.0 + jnp.exp(-v))


def unit(v):
    return v * lax.rsqrt(jnp.sum(v * v, axis=-1, keepdims=True) + 1e-06)


def quad_rows(wide, rows):
    own = lax.broadcasted_iota(jnp.int32, (rows, 128), 0) % 16 // 4
    out = wide[:, 0:128]
    for q in range(1, 4):
        out = jnp.where(own == q, wide[:, 128 * q : 128 * q + 128], out)
    return out


def masks():
    r = lax.broadcasted_iota(jnp.int32, (128, 128), 0)
    c = lax.broadcasted_iota(jnp.int32, (128, 128), 1)
    same = r // 4 == c // 4
    return r == c, same & (c < r), same & (c <= r)


def as_row(col, eye):
    return jnp.sum(jnp.where(eye, col, 0.0), axis=0, keepdims=True)


def ratios(c_col, c_row, keep):
    return jnp.where(keep, jnp.exp(jnp.where(keep, c_col - c_row, 0.0)), 0.0)


def nilpotent(a):
    ab = a.astype(BF16)
    square = mm(ab, ab)
    return square - a - mm(ab, square.astype(BF16))


def main_kernel(
    n,
    tokens, pre_gain, wq, wk, wv, wg, beta_t, decay_t, decay_log, head_gain, out_w, saved,
    ekeys, evals, erates, edecays, accepted,
    state, mixed_in,
    tok, x, w, ow, wt, state_b, ek, ev, k1b, r1, rq, k2b, q2b, v2, gates, tot, proj, scal, ssq, att,
    part, psend, precv, msend,
    tok_sem, ow_sem, s_sem, w_sem, tsend, trecv, gsend, grecv, xsend, xrecv, osend, orecv,
):
    me = lax.axis_index("kv")
    core = lax.axis_index("tp")
    width = n * 128

    load_tok = pltpu.make_async_copy(tokens, tok, tok_sem)
    load_ow = pltpu.make_async_copy(out_w, ow, ow_sem)
    load_tok.start()
    load_ow.start()
    load_s = [pltpu.make_async_copy(saved.at[pl.ds(4 * t, 4)], state.at[pl.ds(4 * t, 4)], s_sem.at[t]) for t in range(8)]
    for c in load_s:
        c.start()
    load_w = [pltpu.make_async_copy(src, w.at[i], w_sem.at[i]) for i, src in enumerate((wq, wk, wv, wg))]
    for c in load_w:
        c.start()

    barrier = pltpu.get_barrier_semaphore()
    for d in range(1, n):
        pl.semaphore_signal(barrier, inc=1, device_id={"kv": lax.rem(me + d, n), "tp": core}, device_id_type=MESH)
    pl.semaphore_signal(barrier, inc=1, device_id={"kv": me, "tp": 1 - core}, device_id_type=MESH)

    eye, strict, incl = masks()
    load_ow.wait()
    wt[pl.ds(me, 1)] = mm_nt(jnp.where(eye, 1.0, 0.0).astype(BF16), ow[...]).astype(BF16)[None]
    load_tok.wait()
    x[pl.ds(me, 1)] = tok[pl.ds(pl.multiple_of(me * 128, 128), 128), :][None]

    pl.semaphore_wait(barrier, n)

    def to_peer(src, dst, ssem, rsem, peer):
        return pltpu.make_async_remote_copy(
            src_ref=src, dst_ref=dst, send_sem=ssem, recv_sem=rsem,
            device_id={"kv": peer, "tp": core}, device_id_type=MESH,
        )

    def send_tok(d):
        peer = lax.rem(me + d, n)
        rows = pl.ds(pl.multiple_of(peer * 128, 128), 128)
        return to_peer(tok.at[rows, :], x.at[me], tsend.at[d], trecv.at[me], peer)

    step_a, step_b = 1 + 3 * core, 4 - 3 * core
    at_a, at_b = lax.rem(me // step_a, 4), lax.rem(me // step_b, 4)

    def place(da, db):
        return lax.rem(at_a + da + 4, 4) * step_a + lax.rem(at_b + db + 4, 4) * step_b

    sent = []

    def part_of(block, side):
        return wt.at[block] if side is None else wt.at[block, pl.ds(64 * side, 64)]

    def pass_on(block, side, peer):
        copy = to_peer(
            part_of(block, side), part_of(block, side), gsend.at[len(sent)], grecv.at[block, 1 if side == 1 else 0], peer
        )
        copy.start()
        sent.append(copy)

    def arrived(block, side):
        to_peer(part_of(block, side), part_of(block, side), gsend.at[0], grecv.at[block, 1 if side == 1 else 0], me).wait_recv()

    def to_b(da):
        for db in (1, -1):
            pass_on(place(da, 0), None, place(0, db))

    def relay_b(da):
        for db in (1, -1):
            arrived(place(da, db), None)
            pass_on(place(da, db), 1 if db == 1 else 0, place(0, -db))

    def gather_first():
        for da in (1, -1):
            pass_on(me, None, place(da, 0))
        to_b(0)

    def gather_second():
        for da in (1, -1):
            arrived(place(da, 0), None)
            pass_on(place(da, 0), 1 if da == 1 else 0, place(-da, 0))
        to_b(1)
        to_b(-1)

    def gather_third():
        for side in (0, 1):
            arrived(place(2, 0), side)
        to_b(2)
        relay_b(0)

    def gather_last():
        for da in range(4):
            for side in (0, 1):
                arrived(place(da, 2), side)

    for d in range(1, n):
        send_tok(d).start()
    gather_first()

    keys = unit(ekeys[...].astype(F32))
    ek[...] = keys
    ev[...] = evals[...].astype(F32)
    count = accepted[...]
    total = jnp.zeros((4, 32), F32)
    rate_p, cum_p = [], []
    for p in range(4):
        live = jnp.where(p < count, 1.0, 0.0)
        total = total + edecays[p] * live
        rate_p.append(erates[p] * live)
        cum_p.append(total)
    row = lax.broadcasted_iota(jnp.int32, (128, 32), 0)
    seq = lax.broadcasted_iota(jnp.int32, (128, 32), 1)

    def expand(pieces):
        out = jnp.zeros((128, 4), F32)
        for p in range(4):
            pick = jnp.where(row == 4 * seq + p, 1.0, 0.0)
            out = out + lax.dot_general(pick, pieces[p], NT, precision=HIGH, preferred_element_type=F32)
        return out

    rate1 = expand(rate_p)
    cum1 = expand(cum_p)
    tot1 = expand([total] * 4)
    for h in range(4):
        k1b[h] = ek[pl.ds(h, 128, stride=4), :].astype(BF16)
        tot[h] = jnp.broadcast_to(jnp.exp(tot1[:, h : h + 1]), (128, 128))
    for c in load_s:
        c.wait()

    def recall(t, _):
        rows = pl.ds(pl.multiple_of(16 * t, 16), 16)
        for h in range(4):
            wide = jnp.concatenate([state[4 * t + q, h].astype(BF16) for q in range(4)], axis=1)
            r1[h, rows, :] = quad_rows(mm(k1b[h, rows, :], wide), 16)
        return 0

    lax.fori_loop(0, 8, recall, 0)
    gather_second()

    for h in range(4):
        b = rate1[:, h : h + 1]
        c_col = cum1[:, h : h + 1]
        kb = k1b[h]
        a = b * ratios(c_col, as_row(c_col, eye), strict) * mm_nt(kb, kb)
        rhs = b * (ev[pl.ds(h, 128, stride=4), :] - jnp.exp(c_col) * r1[h])
        u = rhs + mm(nilpotent(a).astype(BF16), rhs.astype(BF16))
        r1[h] = u * jnp.exp(tot1[:, h : h + 1] - c_col)

    gather_third()
    own = lax.broadcasted_iota(jnp.int32, (16, 128), 0) // 4

    def fold(t, _):
        rows = pl.ds(pl.multiple_of(16 * t, 16), 16)
        for h in range(4):
            u = r1[h, rows, :]
            wide = jnp.concatenate([jnp.where(own == q, u, 0.0) for q in range(4)], axis=1).astype(BF16)
            step = lax.dot_general(k1b[h, rows, :], wide, TN, preferred_element_type=F32)
            for q in range(4):
                new = state[4 * t + q, h] * tot[h, pl.ds(16 * t + 4 * q, 1), :] + step[:, 128 * q : 128 * q + 128]
                state[4 * t + q, h] = new
                state_b[h, t, :, 128 * q : 128 * q + 128] = new.astype(BF16)
        return 0

    lax.fori_loop(0, 8, fold, 0)
    relay_b(1)
    relay_b(-1)

    for c in load_w:
        c.wait()
    proj[...] = jnp.zeros_like(proj)
    scal[...] = jnp.zeros_like(scal)
    ssq[...] = jnp.zeros_like(ssq)
    for g in range(n // 4):
        group = lax.rem(me // 4 + g, n // 4)
        for i in range(4):
            src = 4 * group + i

            @pl.when(src != me)
            def _():
                to_peer(tok.at[pl.ds(0, 128), :], x.at[src], tsend.at[0], trecv.at[src], src).wait_recv()

        pieces = []
        square = jnp.zeros((128, 128), F32)
        for i in range(4):
            wide = x[pl.ds(4 * group + i, 1)][0].astype(F32)
            square = square + wide * wide
            pieces.append((wide * pre_gain[pl.ds(4 * group + i, 1), :]).astype(BF16))
        scaled = jnp.concatenate(pieces, axis=1)
        ssq[...] += square
        cols = pl.ds(pl.multiple_of(group * 512, 512), 512)
        scal[0] += mm_nt(scaled, beta_t[:, cols])
        scal[1] += mm_nt(scaled, decay_t[:, cols])
        for i in range(4):
            proj[i] += mm(scaled, w[i, cols, :])
    relay_b(2)
    inverse = lax.rsqrt(jnp.sum(ssq[...], axis=1, keepdims=True) / width + 1e-06)
    beta_raw = scal[0] * inverse
    decay_raw = scal[1] * inverse
    rates8 = 1.0 / (1.0 + jnp.exp(-beta_raw))
    soft8 = jnp.maximum(decay_raw, 0.0) + jnp.log1p(jnp.exp(-jnp.abs(decay_raw)))
    for h in range(4):
        lanes = slice(128 * h, 128 * h + 128)
        q2b[h] = (unit(silu(proj[0, :, lanes] * inverse)) * 128 ** (-0.5)).astype(BF16)
        k2b[h] = unit(silu(proj[1, :, lanes] * inverse)).astype(BF16)
        v2[h] = silu(proj[2, :, lanes] * inverse)
        gates[h] = silu(proj[3, :, lanes] * inverse) * head_gain[...]

    def recall_new(t, _):
        rows = pl.ds(pl.multiple_of(16 * t, 16), 16)
        for h in range(4):
            both = jnp.concatenate([k2b[h, rows, :], q2b[h, rows, :]], axis=0)
            out = quad_rows(mm(both, state_b[h, t]), 32)
            r1[h, rows, :] = out[:16]
            rq[h, rows, :] = out[16:]
        return 0

    lax.fori_loop(0, 8, recall_new, 0)

    upper = core > 0
    pos = lax.broadcasted_iota(jnp.int32, (128, 1), 0) % 4
    for h in range(4):
        b = jnp.where(upper, rates8[:, h + 4 : h + 5], rates8[:, h : h + 1])
        g = jnp.where(upper, soft8[:, h + 4 : h + 5], soft8[:, h : h + 1])
        g = -jnp.exp(jnp.full((1, 1), decay_log[0, h], F32)) * g
        c_col = jnp.sum(jnp.where(incl, as_row(g, eye), 0.0), axis=1, keepdims=True)
        ratio = ratios(c_col, as_row(c_col, eye), incl)
        kb = k2b[h]
        a = jnp.where(strict, b * ratio * mm_nt(kb, kb), 0.0)
        seen = ratio * mm_nt(q2b[h], kb)
        seen = seen + mm(seen.astype(BF16), nilpotent(a).astype(BF16))
        grown = jnp.exp(c_col)
        rhs = b * (v2[h] - grown * r1[h])
        reads = grown * rq[h] + mm(seen.astype(BF16), rhs.astype(BF16))
        normed = reads * lax.rsqrt(jnp.mean(reads * reads, axis=-1, keepdims=True) + 1e-06)
        att[:, 128 * h : 128 * h + 128] = (normed * gates[h]).astype(BF16)

    gather_last()
    per = n // 4

    def swap(c):
        rows = pl.ds(c * per, per)
        return pltpu.make_async_remote_copy(
            src_ref=psend.at[rows], dst_ref=precv.at[rows], send_sem=xsend.at[c], recv_sem=xrecv.at[c],
            device_id={"kv": me, "tp": 1 - core}, device_id_type=MESH,
        )

    attended = att[...]
    for c in range(4):
        for i in range(c * per, c * per + per):
            out = mm_nt(wt[i], attended)
            part[i] = out
            psend[i] = out.astype(BF16)
        swap(c).start()
    squares = jnp.zeros((128, 128), F32)
    for c in range(4):
        swap(c).wait_recv()
        for i in range(c * per, c * per + per):
            both = part[i] + precv[i].astype(F32)
            squares = squares + both * both
    factor = lax.rsqrt(jnp.sum(squares, axis=0, keepdims=True) / width + 1e-06)
    half = pl.ds(pl.multiple_of(core * 64, 64), 64)
    for i in range(n):
        both = part[i, half, :] + precv[i, half, :].astype(F32)
        msend[i] = (both * factor).astype(BF16)
    mixed_in[pl.ds(me, 1)] = msend[pl.ds(me, 1)]

    def send_out(d):
        peer = lax.rem(me + d, n)
        return to_peer(msend.at[peer], mixed_in.at[me], osend.at[d], orecv.at[me], peer)

    for d in range(1, n):
        send_out(d).start()
    for d in range(1, n):
        src = lax.rem(me + d, n)
        to_peer(msend.at[me], mixed_in.at[src], osend.at[0], orecv.at[src], src).wait_recv()
    for d in range(1, n):
        send_tok(d).wait_send()
        send_out(d).wait_send()
    for c in range(4):
        swap(c).wait_send()
    for copy in sent:
        copy.wait_send()


def last_kernel(n, state, mixed_in, post_gain, committed, mixed, sem):
    copies = [pltpu.make_async_copy(state.at[pl.ds(8 * t, 8)], committed.at[pl.ds(8 * t, 8)], sem.at[t]) for t in range(4)]
    for c in copies:
        c.start()
    i = lax.broadcasted_iota(jnp.int32, (64, 64), 0)
    j = lax.broadcasted_iota(jnp.int32, (64, 64), 1)
    gain = jnp.sum(jnp.where(i == j, post_gain[...], 0.0), axis=1, keepdims=True)
    for k in range(n):
        mixed[:, 128 * k : 128 * k + 128] = (mixed_in[k].astype(F32) * gain).astype(BF16)
    for c in copies:
        c.wait()


def local(
    n,
    tokens, pre_gain, query_weight, key_weight, value_weight, gate_weight, beta_weight, decay_weight, decay_log,
    head_gain, out_weight, post_gain, saved_state, earlier_keys, earlier_values, earlier_rates, earlier_decays, accepted,
):
    any_spec = pl.BlockSpec(memory_space=pl.ANY)
    vmem = pl.BlockSpec(memory_space=VM)
    smem = pl.BlockSpec(memory_space=pltpu.SMEM)
    dma = pltpu.SemaphoreType.DMA
    heads = (4, 128, 128)
    state, mixed_in = pl.pallas_call(
        functools.partial(main_kernel, n),
        out_shape=(VM(saved_state.shape, F32), VM((n, 64, 128), BF16)),
        in_specs=[any_spec, vmem, any_spec, any_spec, any_spec, any_spec, vmem, vmem, smem, vmem, any_spec, any_spec]
        + [vmem] * 5,
        out_specs=(vmem, vmem),
        scratch_shapes=[
            VM((n * 128, 128), BF16),
            VM((n, 128, 128), BF16),
            VM((4, n * 128, 512), BF16),
            VM((512, 128), BF16),
            VM((n, 128, 512), BF16),
            VM((4, 8, 128, 512), BF16),
            VM((512, 128), F32),
            VM((512, 128), F32),
            VM(heads, BF16),
            VM(heads, F32),
            VM(heads, F32),
            VM(heads, BF16),
            VM(heads, BF16),
            VM(heads, F32),
            VM(heads, F32),
            VM(heads, F32),
            VM((4, 128, 512), F32),
            VM((2, 128, 8), F32),
            VM((128, 128), F32),
            VM((128, 512), BF16),
            VM((n, 128, 128), F32),
            VM((n, 128, 128), BF16),
            VM((n, 128, 128), BF16),
            VM((n, 64, 128), BF16),
            dma, dma, dma((8,)), dma((4,)), dma((n,)), dma((n,)), dma((20,)), dma((n, 2)), dma((4,)), dma((4,)), dma((n,)), dma((n,)),
        ],
        compiler_params=pltpu.CompilerParams(collective_id=0, has_side_effects=True, vmem_limit_bytes=48 << 20),
        name="delta_step",
    )(
        tokens, pre_gain.reshape(n, 128), query_weight, key_weight, value_weight, gate_weight, beta_weight.T,
        decay_weight.T, decay_log.reshape(1, 4), head_gain.reshape(1, 128), out_weight, saved_state,
        earlier_keys.reshape(512, 128), earlier_values.reshape(512, 128), earlier_rates.transpose(1, 2, 0),
        earlier_decays.transpose(1, 2, 0), accepted.reshape(1, 32),
    )
    committed, mixed = pl.pallas_call(
        functools.partial(last_kernel, n),
        out_shape=(jax.ShapeDtypeStruct(saved_state.shape, F32), jax.ShapeDtypeStruct((64, n * 128), BF16)),
        in_specs=[vmem] * 3,
        out_specs=(any_spec, vmem),
        scratch_shapes=[dma((4,))],
        compiler_params=pltpu.CompilerParams(vmem_limit_bytes=16 << 20),
        name="write_out",
    )(state, mixed_in, post_gain.reshape(1, 64))
    return mixed.T, committed


def solution(mesh):
    placed = (
        P("dp", "kv"), P(), P(None, "tp"), P(None, "tp"), P(None, "tp"), P(None, "tp"), P(), P(), P("tp"), P(),
        P("tp", "kv"), P(("kv", "tp")), P(("dp", "kv"), "tp", None, None), P(("dp", "kv"), None, "tp", None),
        P(("dp", "kv"), None, "tp", None), P(("dp", "kv"), None, "tp"), P(("dp", "kv"), None, "tp"), P(("dp", "kv")),
    )
    return jax.shard_map(
        functools.partial(local, mesh.shape["kv"]),
        mesh=mesh,
        in_specs=placed,
        out_specs=(P("dp", ("kv", "tp")), P(("dp", "kv"), "tp", None, None)),
        check_vma=False,
    )
```

```python
import functools

import jax
import jax.numpy as jnp
from jax import lax
from jax.experimental import pallas as pl
from jax.experimental.pallas import tpu as pltpu
from jax.sharding import PartitionSpec as P

MESH = pl.DeviceIdType.MESH
F32 = jnp.float32
BF16 = jnp.bfloat16
HIGH = lax.Precision.HIGHEST
VM = pltpu.VMEM
NT = (((1,), (1,)), ((), ()))
TN = (((0,), (0,)), ((), ()))


def mm(a, b):
    return jnp.dot(a, b, preferred_element_type=F32)


def mm_nt(a, b):
    return lax.dot_general(a, b, NT, preferred_element_type=F32)


def silu(v):
    return v / (1.0 + jnp.exp(-v))


def unit(v):
    return v * lax.rsqrt(jnp.sum(v * v, axis=-1, keepdims=True) + 1e-06)


def quad_rows(wide, rows):
    own = lax.broadcasted_iota(jnp.int32, (rows, 128), 0) % 16 // 4
    out = wide[:, 0:128]
    for q in range(1, 4):
        out = jnp.where(own == q, wide[:, 128 * q : 128 * q + 128], out)
    return out


def masks():
    r = lax.broadcasted_iota(jnp.int32, (128, 128), 0)
    c = lax.broadcasted_iota(jnp.int32, (128, 128), 1)
    same = r // 4 == c // 4
    return r == c, same & (c < r), same & (c <= r)


def as_row(col, eye):
    return jnp.sum(jnp.where(eye, col, 0.0), axis=0, keepdims=True)


def ratios(c_col, c_row, keep):
    return jnp.where(keep, jnp.exp(jnp.where(keep, c_col - c_row, 0.0)), 0.0)


def nilpotent(a):
    ab = a.astype(BF16)
    square = mm(ab, ab)
    return square - a - mm(ab, square.astype(BF16))


def main_kernel(
    n,
    tokens, pre_gain, wq, wk, wv, wg, beta_t, decay_t, decay_log, head_gain, out_w, saved,
    ekeys, evals, erates, edecays, accepted,
    state, mixed_in,
    tok, x, w, ow, wt, state_b, ek, ev, k1b, r1, rq, k2b, q2b, v2, gates, tot, proj, scal, ssq, att,
    part, psend, precv, msend,
    tok_sem, ow_sem, s_sem, w_sem, tsend, trecv, gsend, grecv, xsend, xrecv, osend, orecv, fsend, frecv,
):
    me = lax.axis_index("kv")
    core = lax.axis_index("tp")
    width = n * 128

    load_tok = pltpu.make_async_copy(tokens, tok, tok_sem)
    load_ow = pltpu.make_async_copy(out_w, ow, ow_sem)
    load_tok.start()
    load_ow.start()
    barrier = pltpu.get_barrier_semaphore()
    for d in range(1, n):
        pl.semaphore_signal(barrier, inc=1, device_id={"kv": lax.rem(me + d, n), "tp": core}, device_id_type=MESH)
    pl.semaphore_signal(barrier, inc=1, device_id={"kv": me, "tp": 1 - core}, device_id_type=MESH)

    eye, strict, incl = masks()
    load_tok.wait()
    load_ow.wait()
    load_s = [pltpu.make_async_copy(saved.at[pl.ds(4 * t, 4)], state.at[pl.ds(4 * t, 4)], s_sem.at[t]) for t in range(8)]
    for c in load_s:
        c.start()
    load_w = [pltpu.make_async_copy(src, w.at[i], w_sem.at[i]) for i, src in enumerate((wq, wk, wv, wg))]
    for c in load_w:
        c.start()
    wt[pl.ds(me, 1)] = mm_nt(jnp.where(eye, 1.0, 0.0).astype(BF16), ow[...]).astype(BF16)[None]
    half = pl.ds(pl.multiple_of(core * 64, 64), 64)
    x[pl.ds(me, 1), half, :] = tok[pl.ds(pl.multiple_of(me * 128 + core * 64, 64), 64), :][None]

    pl.semaphore_wait(barrier, n)

    def to_peer(src, dst, ssem, rsem, peer):
        return pltpu.make_async_remote_copy(
            src_ref=src, dst_ref=dst, send_sem=ssem, recv_sem=rsem,
            device_id={"kv": peer, "tp": core}, device_id_type=MESH,
        )

    def send_tok(d):
        peer = lax.rem(me + d, n)
        rows = pl.ds(pl.multiple_of(peer * 128 + core * 64, 64), 64)
        return to_peer(tok.at[rows, :], x.at[me, half, :], tsend.at[d], trecv.at[me], peer)

    def share(g):
        some = x.at[pl.ds(4 * lax.rem(me // 4 + g, n // 4), 4), half, :]
        return pltpu.make_async_remote_copy(
            src_ref=some, dst_ref=some, send_sem=fsend.at[g], recv_sem=frecv.at[g],
            device_id={"kv": me, "tp": 1 - core}, device_id_type=MESH,
        )

    step_a, step_b = 1 + 3 * core, 4 - 3 * core
    at_a, at_b = lax.rem(me // step_a, 4), lax.rem(me // step_b, 4)

    def place(da, db):
        return lax.rem(at_a + da + 4, 4) * step_a + lax.rem(at_b + db + 4, 4) * step_b

    sent = []

    def part_of(block, side):
        return wt.at[block] if side is None else wt.at[block, pl.ds(64 * side, 64)]

    def pass_on(block, side, peer):
        copy = to_peer(
            part_of(block, side), part_of(block, side), gsend.at[len(sent)], grecv.at[block, 1 if side == 1 else 0], peer
        )
        copy.start()
        sent.append(copy)

    def arrived(block, side):
        to_peer(part_of(block, side), part_of(block, side), gsend.at[0], grecv.at[block, 1 if side == 1 else 0], me).wait_recv()

    def to_b(da):
        for db in (1, -1):
            pass_on(place(da, 0), None, place(0, db))

    def relay_b(da):
        for db in (1, -1):
            arrived(place(da, db), None)
            pass_on(place(da, db), 1 if db == 1 else 0, place(0, -db))

    def gather_second():
        for da in (1, -1):
            arrived(place(da, 0), None)
            pass_on(place(da, 0), 1 if da == 1 else 0, place(-da, 0))
        to_b(1)
        to_b(-1)

    def gather_third():
        for side in (0, 1):
            arrived(place(2, 0), side)
        to_b(2)
        relay_b(0)

    def gather_last():
        for da in range(4):
            for side in (0, 1):
                arrived(place(da, 2), side)

    for da in (1, -1):
        pass_on(me, None, place(da, 0))
    for d in range(1, n):
        send_tok(d).start()
    to_b(0)

    keys = unit(ekeys[...].astype(F32))
    ek[...] = keys
    ev[...] = evals[...].astype(F32)
    count = accepted[...]
    total = jnp.zeros((4, 32), F32)
    rate_p, cum_p = [], []
    for p in range(4):
        live = jnp.where(p < count, 1.0, 0.0)
        total = total + edecays[p] * live
        rate_p.append(erates[p] * live)
        cum_p.append(total)
    row = lax.broadcasted_iota(jnp.int32, (128, 32), 0)
    seq = lax.broadcasted_iota(jnp.int32, (128, 32), 1)

    def expand(pieces):
        out = jnp.zeros((128, 4), F32)
        for p in range(4):
            pick = jnp.where(row == 4 * seq + p, 1.0, 0.0)
            out = out + lax.dot_general(pick, pieces[p], NT, precision=HIGH, preferred_element_type=F32)
        return out

    rate1 = expand(rate_p)
    cum1 = expand(cum_p)
    tot1 = expand([total] * 4)
    for h in range(4):
        k1b[h] = ek[pl.ds(h, 128, stride=4), :].astype(BF16)
        tot[h] = jnp.broadcast_to(jnp.exp(tot1[:, h : h + 1]), (128, 128))
    for c in load_s:
        c.wait()

    def recall(t, _):
        rows = pl.ds(pl.multiple_of(16 * t, 16), 16)
        for h in range(4):
            wide = jnp.concatenate([state[4 * t + q, h].astype(BF16) for q in range(4)], axis=1)
            r1[h, rows, :] = quad_rows(mm(k1b[h, rows, :], wide), 16)
        return 0

    lax.fori_loop(0, 8, recall, 0)

    for h in range(4):
        b = rate1[:, h : h + 1]
        c_col = cum1[:, h : h + 1]
        kb = k1b[h]
        a = b * ratios(c_col, as_row(c_col, eye), strict) * mm_nt(kb, kb)
        rhs = b * (ev[pl.ds(h, 128, stride=4), :] - jnp.exp(c_col) * r1[h])
        u = rhs + mm(nilpotent(a).astype(BF16), rhs.astype(BF16))
        r1[h] = u * jnp.exp(tot1[:, h : h + 1] - c_col)

    gather_second()
    own = lax.broadcasted_iota(jnp.int32, (16, 128), 0) // 4

    def fold(t, _):
        rows = pl.ds(pl.multiple_of(16 * t, 16), 16)
        for h in range(4):
            u = r1[h, rows, :]
            wide = jnp.concatenate([jnp.where(own == q, u, 0.0) for q in range(4)], axis=1).astype(BF16)
            step = lax.dot_general(k1b[h, rows, :], wide, TN, preferred_element_type=F32)
            for q in range(4):
                new = state[4 * t + q, h] * tot[h, pl.ds(16 * t + 4 * q, 1), :] + step[:, 128 * q : 128 * q + 128]
                state[4 * t + q, h] = new
                state_b[h, t, :, 128 * q : 128 * q + 128] = new.astype(BF16)
        return 0

    lax.fori_loop(0, 8, fold, 0)
    for g in range(n // 4):
        group = lax.rem(me // 4 + g, n // 4)
        for i in range(4):
            src = 4 * group + i

            @pl.when(src != me)
            def _():
                to_peer(tok.at[pl.ds(0, 64), :], x.at[src, half, :], tsend.at[0], trecv.at[src], src).wait_recv()

        share(g).start()
    gather_third()

    for c in load_w:
        c.wait()
    proj[...] = jnp.zeros_like(proj)
    scal[...] = jnp.zeros_like(scal)
    ssq[...] = jnp.zeros_like(ssq)
    for g in range(n // 4):
        group = lax.rem(me // 4 + g, n // 4)
        share(g).wait_recv()
        pieces = []
        square = jnp.zeros((128, 128), F32)
        for i in range(4):
            wide = x[pl.ds(4 * group + i, 1)][0].astype(F32)
            square = square + wide * wide
            pieces.append((wide * pre_gain[pl.ds(4 * group + i, 1), :]).astype(BF16))
        scaled = jnp.concatenate(pieces, axis=1)
        ssq[...] += square
        cols = pl.ds(pl.multiple_of(group * 512, 512), 512)
        scal[0] += mm_nt(scaled, beta_t[:, cols])
        scal[1] += mm_nt(scaled, decay_t[:, cols])
        for i in range(4):
            proj[i] += mm(scaled, w[i, cols, :])
    relay_b(1)
    relay_b(-1)
    inverse = lax.rsqrt(jnp.sum(ssq[...], axis=1, keepdims=True) / width + 1e-06)
    beta_raw = scal[0] * inverse
    decay_raw = scal[1] * inverse
    rates8 = 1.0 / (1.0 + jnp.exp(-beta_raw))
    soft8 = jnp.maximum(decay_raw, 0.0) + jnp.log1p(jnp.exp(-jnp.abs(decay_raw)))
    for h in range(4):
        lanes = slice(128 * h, 128 * h + 128)
        q2b[h] = (unit(silu(proj[0, :, lanes] * inverse)) * 128 ** (-0.5)).astype(BF16)
        k2b[h] = unit(silu(proj[1, :, lanes] * inverse)).astype(BF16)
        v2[h] = silu(proj[2, :, lanes] * inverse)
        gates[h] = silu(proj[3, :, lanes] * inverse) * head_gain[...]

    def recall_new(t, _):
        rows = pl.ds(pl.multiple_of(16 * t, 16), 16)
        for h in range(4):
            both = jnp.concatenate([k2b[h, rows, :], q2b[h, rows, :]], axis=0)
            out = quad_rows(mm(both, state_b[h, t]), 32)
            r1[h, rows, :] = out[:16]
            rq[h, rows, :] = out[16:]
        return 0

    lax.fori_loop(0, 8, recall_new, 0)
    relay_b(2)

    upper = core > 0
    pos = lax.broadcasted_iota(jnp.int32, (128, 1), 0) % 4
    for h in range(4):
        b = jnp.where(upper, rates8[:, h + 4 : h + 5], rates8[:, h : h + 1])
        g = jnp.where(upper, soft8[:, h + 4 : h + 5], soft8[:, h : h + 1])
        g = -jnp.exp(jnp.full((1, 1), decay_log[0, h], F32)) * g
        c_col = jnp.sum(jnp.where(incl, as_row(g, eye), 0.0), axis=1, keepdims=True)
        ratio = ratios(c_col, as_row(c_col, eye), incl)
        kb = k2b[h]
        a = jnp.where(strict, b * ratio * mm_nt(kb, kb), 0.0)
        seen = ratio * mm_nt(q2b[h], kb)
        seen = seen + mm(seen.astype(BF16), nilpotent(a).astype(BF16))
        grown = jnp.exp(c_col)
        rhs = b * (v2[h] - grown * r1[h])
        reads = grown * rq[h] + mm(seen.astype(BF16), rhs.astype(BF16))
        normed = reads * lax.rsqrt(jnp.mean(reads * reads, axis=-1, keepdims=True) + 1e-06)
        att[:, 128 * h : 128 * h + 128] = (normed * gates[h]).astype(BF16)

    gather_last()
    per = n // 4

    def swap(c):
        rows = pl.ds(c * per, per)
        return pltpu.make_async_remote_copy(
            src_ref=psend.at[rows], dst_ref=precv.at[rows], send_sem=xsend.at[c], recv_sem=xrecv.at[c],
            device_id={"kv": me, "tp": 1 - core}, device_id_type=MESH,
        )

    attended = att[...]
    for c in range(4):
        for i in range(c * per, c * per + per):
            out = mm_nt(wt[i], attended)
            part[i] = out
            psend[i] = out.astype(BF16)
        swap(c).start()
    squares = jnp.zeros((128, 128), F32)
    for c in range(4):
        swap(c).wait_recv()
        for i in range(c * per, c * per + per):
            both = part[i] + precv[i].astype(F32)
            squares = squares + both * both
    factor = lax.rsqrt(jnp.sum(squares, axis=0, keepdims=True) / width + 1e-06)
    for i in range(n):
        both = part[i, half, :] + precv[i, half, :].astype(F32)
        msend[i] = (both * factor).astype(BF16)
    mixed_in[pl.ds(me, 1)] = msend[pl.ds(me, 1)]

    def send_out(d):
        peer = lax.rem(me + d, n)
        return to_peer(msend.at[peer], mixed_in.at[me], osend.at[d], orecv.at[me], peer)

    for d in range(1, n):
        send_out(d).start()
    for d in range(1, n):
        src = lax.rem(me + d, n)
        to_peer(msend.at[me], mixed_in.at[src], osend.at[0], orecv.at[src], src).wait_recv()
    for d in range(1, n):
        send_tok(d).wait_send()
        send_out(d).wait_send()
    for c in range(4):
        swap(c).wait_send()
    for g in range(n // 4):
        share(g).wait_send()
    for copy in sent:
        copy.wait_send()


def last_kernel(n, state, mixed_in, post_gain, committed, mixed, sem):
    copies = [pltpu.make_async_copy(state.at[pl.ds(8 * t, 8)], committed.at[pl.ds(8 * t, 8)], sem.at[t]) for t in range(4)]
    for c in copies:
        c.start()
    i = lax.broadcasted_iota(jnp.int32, (64, 64), 0)
    j = lax.broadcasted_iota(jnp.int32, (64, 64), 1)
    gain = jnp.sum(jnp.where(i == j, post_gain[...], 0.0), axis=1, keepdims=True)
    for k in range(n):
        mixed[:, 128 * k : 128 * k + 128] = (mixed_in[k].astype(F32) * gain).astype(BF16)
    for c in copies:
        c.wait()


def local(
    n,
    tokens, pre_gain, query_weight, key_weight, value_weight, gate_weight, beta_weight, decay_weight, decay_log,
    head_gain, out_weight, post_gain, saved_state, earlier_keys, earlier_values, earlier_rates, earlier_decays, accepted,
):
    any_spec = pl.BlockSpec(memory_space=pl.ANY)
    vmem = pl.BlockSpec(memory_space=VM)
    smem = pl.BlockSpec(memory_space=pltpu.SMEM)
    dma = pltpu.SemaphoreType.DMA
    heads = (4, 128, 128)
    state, mixed_in = pl.pallas_call(
        functools.partial(main_kernel, n),
        out_shape=(VM(saved_state.shape, F32), VM((n, 64, 128), BF16)),
        in_specs=[any_spec, vmem, any_spec, any_spec, any_spec, any_spec, vmem, vmem, smem, vmem, any_spec, any_spec]
        + [vmem] * 5,
        out_specs=(vmem, vmem),
        scratch_shapes=[
            VM((n * 128, 128), BF16),
            VM((n, 128, 128), BF16),
            VM((4, n * 128, 512), BF16),
            VM((512, 128), BF16),
            VM((n, 128, 512), BF16),
            VM((4, 8, 128, 512), BF16),
            VM((512, 128), F32),
            VM((512, 128), F32),
            VM(heads, BF16),
            VM(heads, F32),
            VM(heads, F32),
            VM(heads, BF16),
            VM(heads, BF16),
            VM(heads, F32),
            VM(heads, F32),
            VM(heads, F32),
            VM((4, 128, 512), F32),
            VM((2, 128, 8), F32),
            VM((128, 128), F32),
            VM((128, 512), BF16),
            VM((n, 128, 128), F32),
            VM((n, 128, 128), BF16),
            VM((n, 128, 128), BF16),
            VM((n, 64, 128), BF16),
            dma, dma, dma((8,)), dma((4,)), dma((n,)), dma((n,)), dma((20,)), dma((n, 2)), dma((4,)), dma((4,)), dma((n,)), dma((n,)), dma((4,)), dma((4,)),
        ],
        compiler_params=pltpu.CompilerParams(collective_id=0, has_side_effects=True, vmem_limit_bytes=48 << 20),
        name="delta_step",
    )(
        tokens, pre_gain.reshape(n, 128), query_weight, key_weight, value_weight, gate_weight, beta_weight.T,
        decay_weight.T, decay_log.reshape(1, 4), head_gain.reshape(1, 128), out_weight, saved_state,
        earlier_keys.reshape(512, 128), earlier_values.reshape(512, 128), earlier_rates.transpose(1, 2, 0),
        earlier_decays.transpose(1, 2, 0), accepted.reshape(1, 32),
    )
    committed, mixed = pl.pallas_call(
        functools.partial(last_kernel, n),
        out_shape=(jax.ShapeDtypeStruct(saved_state.shape, F32), jax.ShapeDtypeStruct((64, n * 128), BF16)),
        in_specs=[vmem] * 3,
        out_specs=(any_spec, vmem),
        scratch_shapes=[dma((4,))],
        compiler_params=pltpu.CompilerParams(vmem_limit_bytes=16 << 20),
        name="write_out",
    )(state, mixed_in, post_gain.reshape(1, 64))
    return mixed.T, committed


def solution(mesh):
    placed = (
        P("dp", "kv"), P(), P(None, "tp"), P(None, "tp"), P(None, "tp"), P(None, "tp"), P(), P(), P("tp"), P(),
        P("tp", "kv"), P(("kv", "tp")), P(("dp", "kv"), "tp", None, None), P(("dp", "kv"), None, "tp", None),
        P(("dp", "kv"), None, "tp", None), P(("dp", "kv"), None, "tp"), P(("dp", "kv"), None, "tp"), P(("dp", "kv")),
    )
    return jax.shard_map(
        functools.partial(local, mesh.shape["kv"]),
        mesh=mesh,
        in_specs=placed,
        out_specs=(P("dp", ("kv", "tp")), P(("dp", "kv"), "tp", None, None)),
        check_vma=False,
    )
```

```python
import functools

import jax
import jax.numpy as jnp
from jax import lax
from jax.experimental import pallas as pl
from jax.experimental.pallas import tpu as pltpu
from jax.sharding import PartitionSpec as P

MESH = pl.DeviceIdType.MESH
F32 = jnp.float32
BF16 = jnp.bfloat16
HIGH = lax.Precision.HIGHEST
VM = pltpu.VMEM
NT = (((1,), (1,)), ((), ()))
TN = (((0,), (0,)), ((), ()))


def mm(a, b):
    return jnp.dot(a, b, preferred_element_type=F32)


def mm_nt(a, b):
    return lax.dot_general(a, b, NT, preferred_element_type=F32)


def silu(v):
    return v / (1.0 + jnp.exp(-v))


def unit(v):
    return v * lax.rsqrt(jnp.sum(v * v, axis=-1, keepdims=True) + 1e-06)


def quad_rows(wide, rows):
    own = lax.broadcasted_iota(jnp.int32, (rows, 128), 0) % 16 // 4
    out = wide[:, 0:128]
    for q in range(1, 4):
        out = jnp.where(own == q, wide[:, 128 * q : 128 * q + 128], out)
    return out


def masks():
    r = lax.broadcasted_iota(jnp.int32, (128, 128), 0)
    c = lax.broadcasted_iota(jnp.int32, (128, 128), 1)
    same = r // 4 == c // 4
    return r == c, same, same & (c < r), same & (c <= r)


def as_row(col, eye):
    return jnp.sum(jnp.where(eye, col, 0.0), axis=0, keepdims=True)


def ratios(c_col, c_row, keep):
    return jnp.where(keep, jnp.exp(jnp.where(keep, c_col - c_row, 0.0)), 0.0)


def nilpotent(a):
    ab = a.astype(BF16)
    square = mm(ab, ab)
    return square - a - mm(ab, square.astype(BF16))


def main_kernel(
    n,
    tokens, out_w, saved, wq, wk, wv, wg,
    ekeys_in, evals_in, erates_in, edecays_in, accepted_in, pre_gain_in, beta_in, decay_in, decay_log_in, head_gain_in,
    state, mixed_in, sums, k1b, u1, tot,
    ekeys, evals, erates, edecays, accepted, pre_gain, beta_t, decay_t, decay_log, head_gain,
    tok, x, w, ow, wt, state_b, ek, ev, r1, rq, k2b, q2b, v2, gates, proj, scal, ssq, att,
    part, psend, precv, msend,
    tok_sem, ow_sem, s_sem, w_sem, small_sem, tsend, trecv, gsend, grecv, xsend, xrecv, osend, orecv, fsend, frecv,
    asend, arecv, ssend, srecv,
):
    me = lax.axis_index("kv")
    core = lax.axis_index("tp")
    width = n * 128

    barrier = pltpu.get_barrier_semaphore()
    for d in range(1, n):
        pl.semaphore_signal(barrier, inc=1, device_id={"kv": lax.rem(me + d, n), "tp": core}, device_id_type=MESH)
    pl.semaphore_signal(barrier, inc=1, device_id={"kv": me, "tp": 1 - core}, device_id_type=MESH)

    load_tok = pltpu.make_async_copy(tokens, tok, tok_sem)
    load_ow = pltpu.make_async_copy(out_w, ow, ow_sem)
    load_ow.start()
    load_tok.start()
    small = (
        (ekeys_in, ekeys), (evals_in, evals), (erates_in, erates), (edecays_in, edecays), (accepted_in, accepted),
        (pre_gain_in, pre_gain), (beta_in, beta_t), (decay_in, decay_t), (decay_log_in, decay_log), (head_gain_in, head_gain),
    )
    load_small = [pltpu.make_async_copy(src, dst, small_sem.at[i]) for i, (src, dst) in enumerate(small)]
    for c in load_small:
        c.start()

    def load_s(t):
        some = pl.ds(4 * t, 4)
        return pltpu.make_async_copy(saved.at[some], state.at[some], s_sem.at[t])

    load_w = [pltpu.make_async_copy(src, w.at[i], w_sem.at[i]) for i, src in enumerate((wq, wk, wv, wg))]

    eye, same, strict, incl = masks()
    load_ow.wait()
    load_tok.wait()
    for c in load_small:
        c.wait()
    for t in range(8):
        load_s(t).start()
    wt[pl.ds(me, 1)] = mm_nt(jnp.where(eye, 1.0, 0.0).astype(BF16), ow[...]).astype(BF16)[None]
    half = pl.ds(pl.multiple_of(core * 64, 64), 64)
    x[pl.ds(me, 1), half, :] = tok[pl.ds(pl.multiple_of(me * 128 + core * 64, 64), 64), :][None]

    keys = unit(ekeys[...].astype(F32))
    ek[...] = keys
    ev[...] = evals[...].astype(F32)
    count = accepted[...]
    total = jnp.zeros((4, 32), F32)
    rate_p, cum_p = [], []
    for p in range(4):
        live = jnp.where(p < count, 1.0, 0.0)
        total = total + edecays[p] * live
        rate_p.append(erates[p] * live)
        cum_p.append(total)
    row = lax.broadcasted_iota(jnp.int32, (128, 32), 0)
    seq = lax.broadcasted_iota(jnp.int32, (128, 32), 1)

    def expand(pieces):
        out = jnp.zeros((128, 4), F32)
        for p in range(4):
            pick = jnp.where(row == 4 * seq + p, 1.0, 0.0)
            out = out + lax.dot_general(pick, pieces[p], NT, precision=HIGH, preferred_element_type=F32)
        return out

    rate1 = expand(rate_p)
    cum1 = expand(cum_p)
    tot1 = expand([total] * 4)
    pl.semaphore_wait(barrier, n)

    def to_peer(src, dst, ssem, rsem, peer):
        return pltpu.make_async_remote_copy(
            src_ref=src, dst_ref=dst, send_sem=ssem, recv_sem=rsem,
            device_id={"kv": peer, "tp": core}, device_id_type=MESH,
        )

    def send_tok(d):
        peer = lax.rem(me + d, n)
        rows = pl.ds(pl.multiple_of(peer * 128 + core * 64, 64), 64)
        return to_peer(tok.at[rows, :], x.at[me, half, :], tsend, trecv.at[me // 4], peer)

    def share(g):
        some = x.at[pl.ds(4 * lax.rem(me // 4 + g, n // 4), 4), half, :]
        return pltpu.make_async_remote_copy(
            src_ref=some, dst_ref=some, send_sem=fsend, recv_sem=frecv.at[g],
            device_id={"kv": me, "tp": 1 - core}, device_id_type=MESH,
        )

    at_z, at_y = me // 4, lax.rem(me, 4)
    pair = me + 1 - 2 * lax.rem(at_y, 2)

    def place(dz, side):
        return lax.rem(at_z + dz, n // 4) * 4 + at_y + side * (3 - 2 * at_y)

    def pass_on(block, peer):
        return to_peer(wt.at[block], wt.at[block], gsend, grecv.at[block], peer)

    def arrived(block):
        pass_on(block, me).wait_recv()

    far = [dz for dz in (2, 1, 3) if dz < n // 4]

    def gather_first():
        pass_on(me, place(0, 1)).start()
        for dz in far:
            pass_on(me, place(dz, 0)).start()

    def gather_second():
        arrived(place(0, 1))
        for dz in far:
            along, across = place(dz, 0), place(0, 1)
            arrived(along)
            pass_on(across + core * (along - across), along + core * (across - along)).start()

    for d in range(1, n):
        send_tok(d).start()
    gather_first()
    for c in load_w:
        c.start()

    for h in range(4):
        k1b[h] = ek[pl.ds(h, 128, stride=4), :].astype(BF16)
        tot[h] = jnp.broadcast_to(jnp.exp(tot1[:, h : h + 1]), (128, 128))

    def recall(t, _):
        load_s(t).wait()
        rows = pl.ds(pl.multiple_of(16 * t, 16), 16)
        for h in range(4):
            wide = jnp.concatenate([state[4 * t + q, h].astype(BF16) for q in range(4)], axis=1)
            state_b[h, t] = wide
            r1[h, rows, :] = quad_rows(mm(k1b[h, rows, :], wide), 16)
        return 0

    lax.fori_loop(0, 8, recall, 0)

    for h in range(4):
        b = rate1[:, h : h + 1]
        c_col = cum1[:, h : h + 1]
        kb = k1b[h]
        a = b * ratios(c_col, as_row(c_col, eye), strict) * mm_nt(kb, kb)
        rhs = b * (ev[pl.ds(h, 128, stride=4), :] - jnp.exp(c_col) * r1[h])
        u = rhs + mm(nilpotent(a).astype(BF16), rhs.astype(BF16))
        u1[h] = u * jnp.exp(tot1[:, h : h + 1] - c_col)

    def collect(g):
        group = lax.rem(me // 4 + g, n // 4)
        count = 4 if g else 3
        rows = tok.at[pl.ds(0, 64 * count), :]
        to_peer(rows, rows, tsend, trecv.at[group], me).wait_recv()
        share(g).start()

    def project(g):
        group = lax.rem(me // 4 + g, n // 4)
        share(g).wait_recv()
        pieces = []
        square = jnp.zeros((128, 128), F32)
        for i in range(4):
            wide = x[pl.ds(4 * group + i, 1)][0].astype(F32)
            square = square + wide * wide
            pieces.append((wide * pre_gain[pl.ds(4 * group + i, 1), :]).astype(BF16))
        scaled = jnp.concatenate(pieces, axis=1)
        cols = pl.ds(pl.multiple_of(group * 512, 512), 512)
        beta = mm_nt(scaled, beta_t[:, cols])
        decay = mm_nt(scaled, decay_t[:, cols])
        ssq[...] = square if g == 0 else ssq[...] + square
        scal[0] = beta if g == 0 else scal[0] + beta
        scal[1] = decay if g == 0 else scal[1] + decay
        for i in range(4):
            out = mm(scaled, w[i, cols, :])
            proj[i] = out if g == 0 else proj[i] + out

    groups = n // 4
    for c in load_w:
        c.wait()
    for g in range(groups):
        collect(g)
        if g > 1:
            project(g - 2)
    for g in range(max(groups - 2, 0), groups):
        project(g)
    inverse = lax.rsqrt(jnp.sum(ssq[...], axis=1, keepdims=True) / width + 1e-06)
    beta_raw = scal[0] * inverse
    decay_raw = scal[1] * inverse
    rates8 = 1.0 / (1.0 + jnp.exp(-beta_raw))
    soft8 = jnp.maximum(decay_raw, 0.0) + jnp.log1p(jnp.exp(-jnp.abs(decay_raw)))
    for h in range(4):
        lanes = slice(128 * h, 128 * h + 128)
        q2b[h] = (unit(silu(proj[0, :, lanes] * inverse)) * 128 ** (-0.5)).astype(BF16)
        k2b[h] = unit(silu(proj[1, :, lanes] * inverse)).astype(BF16)
        v2[h] = silu(proj[2, :, lanes] * inverse)
        gates[h] = silu(proj[3, :, lanes] * inverse) * head_gain[...]

    def recall_new(t, _):
        rows = pl.ds(pl.multiple_of(16 * t, 16), 16)
        for h in range(4):
            both = jnp.concatenate([k2b[h, rows, :], q2b[h, rows, :]], axis=0)
            out = quad_rows(mm(both, state_b[h, t]), 32)
            r1[h, rows, :] = out[:16]
            rq[h, rows, :] = out[16:]
        return 0

    lax.fori_loop(0, 8, recall_new, 0)
    gather_second()

    def to_pair(h):
        two = pl.ds(2 * h, 2)
        return to_peer(att.at[0, two], att.at[1, two], asend, arecv, pair)

    upper = core > 0
    pos = lax.broadcasted_iota(jnp.int32, (128, 1), 0) % 4
    for h in range(4):
        b = jnp.where(upper, rates8[:, h + 4 : h + 5], rates8[:, h : h + 1])
        g = jnp.where(upper, soft8[:, h + 4 : h + 5], soft8[:, h : h + 1])
        g = -jnp.exp(decay_log[:, h : h + 1]) * g
        c_col = jnp.sum(jnp.where(incl, as_row(g, eye), 0.0), axis=1, keepdims=True)
        ratio = ratios(c_col, as_row(c_col, eye), incl)
        kb, kept = k2b[h], tot[h]
        cross = mm_nt(jnp.concatenate([kb, q2b[h]], axis=0), jnp.concatenate([kb, k1b[h]], axis=0))
        a = jnp.where(strict, b * ratio * cross[:128, :128], 0.0)
        seen = ratio * cross[128:, :128]
        past = jnp.concatenate([jnp.where(same, cross[:128, 128:], 0.0), jnp.where(same, cross[128:, 128:], 0.0)], axis=0)
        past = mm(past.astype(BF16), u1[h].astype(BF16))
        recalled = kept * r1[h] + past[:128]
        queried = kept * rq[h] + past[128:]
        seen = seen + mm(seen.astype(BF16), nilpotent(a).astype(BF16))
        grown = jnp.exp(c_col)
        rhs = b * (v2[h] - grown * recalled)
        reads = grown * queried + mm(seen.astype(BF16), rhs.astype(BF16))
        normed = reads * lax.rsqrt(jnp.mean(reads * reads, axis=-1, keepdims=True) + 1e-06)
        att[0, h] = (normed * gates[h]).astype(BF16)
        if h % 2:
            to_pair(h // 2).start()

    def swap(c):
        part_sum = slice(None) if c is None else c
        return pltpu.make_async_remote_copy(
            src_ref=psend.at[part_sum], dst_ref=precv.at[part_sum], send_sem=xsend, recv_sem=xrecv,
            device_id={"kv": me, "tp": 1 - core}, device_id_type=MESH,
        )

    to_peer(att.at[0], att.at[1], asend, arecv, pair).wait()
    attended = jnp.concatenate([jnp.concatenate([att[i, h] for h in range(4)], axis=1) for i in range(2)], axis=0)
    blocks = [(dz, side) for side in range(2) for dz in [0] + far]
    many = n // 4
    for side in range(2):
        for dz in far if side else ():
            arrived(place(dz, side))
        some = jnp.concatenate([wt[pl.ds(place(dz, side), 1)][0] for dz in [0] + far], axis=0)
        out = mm_nt(some, attended).reshape(many, 128, 256)
        rows = pl.ds(side * many, many)
        part[rows] = out
        psend[rows] = out.astype(BF16)
        swap(rows).start()
    swap(None).wait_recv()
    squares = jnp.zeros((128, 256), F32)
    for i in range(n // 2):
        both = part[i] + precv[i].astype(F32)
        squares = squares + both * both
        part[i] = both
    squares = jnp.sum(squares, axis=0, keepdims=True)
    first = lax.broadcasted_iota(jnp.int32, (8, 128), 0) == 0
    sums[pl.ds(me, 1)] = jnp.where(first, squares[:, :128], squares[:, 128:])[None]

    def send_sums(d):
        peer = lax.rem(me + d, n)
        return to_peer(sums.at[me], sums.at[me], ssend, srecv, peer)

    for d in range(1, n):
        send_sums(d).start()
    for i in range(n // 2):
        both = part[i, half, :].astype(BF16)
        msend[0, i] = both[:, :128]
        msend[1, i] = both[:, 128:]
    mixed_in[pl.ds(me, 1)] = msend[0, 0][None]
    mixed_in[pl.ds(pair, 1)] = msend[1, 0][None]
    for i, (dz, side) in enumerate(blocks):
        if i:
            peer = place(dz, side)
            to_peer(msend.at[0, i], mixed_in.at[me], osend, orecv, peer).start()
            to_peer(msend.at[1, i], mixed_in.at[pair], osend, orecv, peer).start()
    others = pl.ds(0, n - 2)
    to_peer(mixed_in.at[others], mixed_in.at[others], osend, orecv, me).wait()
    others = pl.ds(0, n - 1)
    to_peer(sums.at[others], sums.at[others], ssend, srecv, me).wait()
    rows = tok.at[pl.ds(0, 64 * (n - 1)), :]
    to_peer(rows, rows, tsend, tsend, me).wait_send()
    mine = x.at[:, half, :]
    to_peer(mine, mine, fsend, fsend, me).wait_send()
    others = pl.ds(0, 1 + 2 * len(far))
    to_peer(wt.at[others], wt.at[others], gsend, gsend, me).wait_send()
    swap(None).wait_send()


def last_kernel(n, state, k1b, u1, tot, mixed_in, sums, post_gain, committed, mixed, new, rows_out, sem, mixed_sem):
    i = lax.broadcasted_iota(jnp.int32, (64, 64), 0)
    j = lax.broadcasted_iota(jnp.int32, (64, 64), 1)
    gain = jnp.sum(jnp.where(i == j, post_gain[...], 0.0), axis=1, keepdims=True)
    for k in range(n):
        total = sums[k, 0:1, :] + sums[k + 1 - 2 * (k % 2), 1:2, :]
        factor = lax.rsqrt(total / (n * 128) + 1e-06)
        rows_out[:, 128 * k : 128 * k + 128] = (mixed_in[k].astype(F32) * factor * gain).astype(BF16)
    write_mixed = pltpu.make_async_copy(rows_out, mixed, mixed_sem)
    write_mixed.start()
    own = lax.broadcasted_iota(jnp.int32, (16, 128), 0) // 4

    def write(t):
        some = pl.ds(4 * t, 4)
        return pltpu.make_async_copy(new.at[some], committed.at[some], sem.at[t])

    def fold(t, _):
        rows = pl.ds(pl.multiple_of(16 * t, 16), 16)
        for h in range(4):
            u = u1[h, rows, :]
            wide = jnp.concatenate([jnp.where(own == q, u, 0.0) for q in range(4)], axis=1).astype(BF16)
            step = lax.dot_general(k1b[h, rows, :], wide, TN, preferred_element_type=F32)
            for q in range(4):
                kept = state[4 * t + q, h] * tot[h, pl.ds(16 * t + 4 * q, 1), :]
                new[4 * t + q, h] = kept + step[:, 128 * q : 128 * q + 128]
        write(t).start()
        return 0

    lax.fori_loop(0, 8, fold, 0)
    for t in range(8):
        write(t).wait()
    write_mixed.wait()


def local(
    n,
    tokens, pre_gain, query_weight, key_weight, value_weight, gate_weight, beta_weight, decay_weight, decay_log,
    head_gain, out_weight, post_gain, saved_state, earlier_keys, earlier_values, earlier_rates, earlier_decays, accepted,
):
    any_spec = pl.BlockSpec(memory_space=pl.ANY)
    vmem = pl.BlockSpec(memory_space=VM)
    dma = pltpu.SemaphoreType.DMA
    heads = (4, 128, 128)
    state, mixed_in, sums, k1b, u1, tot = pl.pallas_call(
        functools.partial(main_kernel, n),
        out_shape=(VM(saved_state.shape, F32), VM((n, 64, 128), BF16), VM((n, 8, 128), F32), VM(heads, BF16), VM(heads, F32), VM(heads, F32)),
        in_specs=[any_spec] * 17,
        out_specs=(vmem,) * 6,
        scratch_shapes=[
            VM((512, 128), BF16),
            VM((512, 128), BF16),
            VM((4, 4, 32), F32),
            VM((4, 4, 32), F32),
            VM((1, 32), jnp.int32),
            VM((n, 128), F32),
            VM((8, n * 128), BF16),
            VM((8, n * 128), BF16),
            VM((1, 4), F32),
            VM((1, 128), F32),
            VM((n * 128, 128), BF16),
            VM((n, 128, 128), BF16),
            VM((4, n * 128, 512), BF16),
            VM((512, 128), BF16),
            VM((n, 128, 512), BF16),
            VM((4, 8, 128, 512), BF16),
            VM((512, 128), F32),
            VM((512, 128), F32),
            VM(heads, F32),
            VM(heads, F32),
            VM(heads, BF16),
            VM(heads, BF16),
            VM(heads, F32),
            VM(heads, F32),
            VM((4, 128, 512), F32),
            VM((2, 128, 8), F32),
            VM((128, 128), F32),
            VM((2, 4, 128, 128), BF16),
            VM((n // 2, 128, 256), F32),
            VM((n // 2, 128, 256), BF16),
            VM((n // 2, 128, 256), BF16),
            VM((2, n // 2, 64, 128), BF16),
            dma, dma, dma((8,)), dma((4,)), dma((10,)),
            dma, dma((n // 4,)), dma, dma((n,)), dma, dma, dma, dma, dma, dma((n // 4,)), dma, dma, dma, dma,
        ],
        compiler_params=pltpu.CompilerParams(collective_id=0, has_side_effects=True, vmem_limit_bytes=48 << 20),
        name="delta_step",
    )(
        tokens, out_weight, saved_state, query_weight, key_weight, value_weight, gate_weight,
        earlier_keys.reshape(512, 128), earlier_values.reshape(512, 128), earlier_rates.transpose(1, 2, 0),
        earlier_decays.transpose(1, 2, 0), accepted.reshape(1, 32), pre_gain.reshape(n, 128), beta_weight.T,
        decay_weight.T, decay_log.reshape(1, 4), head_gain.reshape(1, 128),
    )
    committed, mixed = pl.pallas_call(
        functools.partial(last_kernel, n),
        out_shape=(jax.ShapeDtypeStruct(saved_state.shape, F32), jax.ShapeDtypeStruct((64, n * 128), BF16)),
        in_specs=[vmem] * 7,
        out_specs=(any_spec, any_spec),
        scratch_shapes=[VM(saved_state.shape, F32), VM((64, n * 128), BF16), dma((8,)), dma],
        compiler_params=pltpu.CompilerParams(vmem_limit_bytes=32 << 20),
        name="write_out",
    )(state, k1b, u1, tot, mixed_in, sums, post_gain.reshape(1, 64))
    return mixed.T, committed


def solution(mesh):
    placed = (
        P("dp", "kv"), P(), P(None, "tp"), P(None, "tp"), P(None, "tp"), P(None, "tp"), P(), P(), P("tp"), P(),
        P("tp", "kv"), P(("kv", "tp")), P(("dp", "kv"), "tp", None, None), P(("dp", "kv"), None, "tp", None),
        P(("dp", "kv"), None, "tp", None), P(("dp", "kv"), None, "tp"), P(("dp", "kv"), None, "tp"), P(("dp", "kv")),
    )
    return jax.shard_map(
        functools.partial(local, mesh.shape["kv"]),
        mesh=mesh,
        in_specs=placed,
        out_specs=(P("dp", ("kv", "tp")), P(("dp", "kv"), "tp", None, None)),
        check_vma=False,
    )
```

```python
import functools

import jax
import jax.numpy as jnp
from jax import lax
from jax.experimental import pallas as pl
from jax.experimental.pallas import tpu as pltpu
from jax.sharding import PartitionSpec as P

MESH = pl.DeviceIdType.MESH
F32 = jnp.float32
BF16 = jnp.bfloat16
HIGH = lax.Precision.HIGHEST
VM = pltpu.VMEM
NT = (((1,), (1,)), ((), ()))
TN = (((0,), (0,)), ((), ()))


def mm(a, b):
    return jnp.dot(a, b, preferred_element_type=F32)


def mm_nt(a, b):
    return lax.dot_general(a, b, NT, preferred_element_type=F32)


def silu(v):
    return v / (1.0 + jnp.exp(-v))


def unit(v):
    return v * lax.rsqrt(jnp.sum(v * v, axis=-1, keepdims=True) + 1e-06)


def quad_rows(wide, rows):
    own = lax.broadcasted_iota(jnp.int32, (rows, 128), 0) % 16 // 4
    out = wide[:, 0:128]
    for q in range(1, 4):
        out = jnp.where(own == q, wide[:, 128 * q : 128 * q + 128], out)
    return out


def masks():
    r = lax.broadcasted_iota(jnp.int32, (128, 128), 0)
    c = lax.broadcasted_iota(jnp.int32, (128, 128), 1)
    same = r // 4 == c // 4
    return r == c, same & (c < r), same & (c <= r)


def as_row(col, eye):
    return jnp.sum(jnp.where(eye, col, 0.0), axis=0, keepdims=True)


def ratios(c_col, c_row, keep):
    return jnp.where(keep, jnp.exp(jnp.where(keep, c_col - c_row, 0.0)), 0.0)


def nilpotent(a):
    ab = a.astype(BF16)
    square = mm(ab, ab)
    return square - a - mm(ab, square.astype(BF16))


def main_kernel(
    n,
    tokens, out_w, saved, wq, wk, wv, wg,
    ekeys_in, evals_in, erates_in, edecays_in, accepted_in, pre_gain_in, beta_in, decay_in, decay_log_in, head_gain_in,
    state, mixed_in, sums,
    ekeys, evals, erates, edecays, accepted, pre_gain, beta_t, decay_t, decay_log, head_gain,
    tok, x, w, ow, wt, state_b, ek, ev, k1b, u1, tot, r1, rq, k2b, q2b, v2, gates, proj, scal, ssq, att,
    part, psend, precv, msend,
    tok_sem, ow_sem, s_sem, w_sem, small_sem, tsend, trecv, gsend, grecv, xsend, xrecv, osend, orecv, fsend, frecv,
    asend, arecv, ssend, srecv,
):
    me = lax.axis_index("kv")
    core = lax.axis_index("tp")
    width = n * 128

    barrier = pltpu.get_barrier_semaphore()
    for d in range(1, n):
        pl.semaphore_signal(barrier, inc=1, device_id={"kv": lax.rem(me + d, n), "tp": core}, device_id_type=MESH)
    pl.semaphore_signal(barrier, inc=1, device_id={"kv": me, "tp": 1 - core}, device_id_type=MESH)

    load_tok = pltpu.make_async_copy(tokens, tok, tok_sem)
    load_ow = pltpu.make_async_copy(out_w, ow, ow_sem)
    load_ow.start()
    load_tok.start()
    small = (
        (ekeys_in, ekeys), (evals_in, evals), (erates_in, erates), (edecays_in, edecays), (accepted_in, accepted),
        (pre_gain_in, pre_gain), (beta_in, beta_t), (decay_in, decay_t), (decay_log_in, decay_log), (head_gain_in, head_gain),
    )
    load_small = [pltpu.make_async_copy(src, dst, small_sem.at[i]) for i, (src, dst) in enumerate(small)]
    for c in load_small:
        c.start()

    def load_s(t):
        some = pl.ds(4 * t, 4)
        return pltpu.make_async_copy(saved.at[some], state.at[some], s_sem.at[t])

    load_w = [pltpu.make_async_copy(src, w.at[i], w_sem.at[i]) for i, src in enumerate((wq, wk, wv, wg))]

    eye, strict, incl = masks()
    load_ow.wait()
    load_tok.wait()
    for c in load_small:
        c.wait()
    for t in range(8):
        load_s(t).start()
    wt[pl.ds(me, 1)] = mm_nt(jnp.where(eye, 1.0, 0.0).astype(BF16), ow[...]).astype(BF16)[None]
    half = pl.ds(pl.multiple_of(core * 64, 64), 64)
    x[pl.ds(me, 1), half, :] = tok[pl.ds(pl.multiple_of(me * 128 + core * 64, 64), 64), :][None]

    keys = unit(ekeys[...].astype(F32))
    ek[...] = keys
    ev[...] = evals[...].astype(F32)
    count = accepted[...]
    total = jnp.zeros((4, 32), F32)
    rate_p, cum_p = [], []
    for p in range(4):
        live = jnp.where(p < count, 1.0, 0.0)
        total = total + edecays[p] * live
        rate_p.append(erates[p] * live)
        cum_p.append(total)
    row = lax.broadcasted_iota(jnp.int32, (128, 32), 0)
    seq = lax.broadcasted_iota(jnp.int32, (128, 32), 1)

    def expand(pieces):
        out = jnp.zeros((128, 4), F32)
        for p in range(4):
            pick = jnp.where(row == 4 * seq + p, 1.0, 0.0)
            out = out + lax.dot_general(pick, pieces[p], NT, precision=HIGH, preferred_element_type=F32)
        return out

    rate1 = expand(rate_p)
    cum1 = expand(cum_p)
    tot1 = expand([total] * 4)
    pl.semaphore_wait(barrier, n)

    def to_peer(src, dst, ssem, rsem, peer):
        return pltpu.make_async_remote_copy(
            src_ref=src, dst_ref=dst, send_sem=ssem, recv_sem=rsem,
            device_id={"kv": peer, "tp": core}, device_id_type=MESH,
        )

    def send_tok(d):
        peer = lax.rem(me + d, n)
        rows = pl.ds(pl.multiple_of(peer * 128 + core * 64, 64), 64)
        return to_peer(tok.at[rows, :], x.at[me, half, :], tsend, trecv.at[me // 4], peer)

    def share(g):
        some = x.at[pl.ds(4 * lax.rem(me // 4 + g, n // 4), 4), half, :]
        return pltpu.make_async_remote_copy(
            src_ref=some, dst_ref=some, send_sem=fsend, recv_sem=frecv.at[g],
            device_id={"kv": me, "tp": 1 - core}, device_id_type=MESH,
        )

    at_z, at_y = me // 4, lax.rem(me, 4)
    pair = me + 1 - 2 * lax.rem(at_y, 2)

    def place(dz, side):
        return lax.rem(at_z + dz, n // 4) * 4 + at_y + side * (3 - 2 * at_y)

    def pass_on(block, peer):
        return to_peer(wt.at[block], wt.at[block], gsend, grecv.at[block], peer)

    def arrived(block):
        pass_on(block, me).wait_recv()

    far = [dz for dz in (2, 1, 3) if dz < n // 4]

    def gather_first(along):
        @pl.when(core == along)
        def _():
            for dz in far:
                pass_on(me, place(dz, 0)).start()

        @pl.when(core != along)
        def _():
            pass_on(me, place(0, 1)).start()

    def gather_second():
        arrived(place(0, 1))
        for dz in far:
            along, across = place(dz, 0), place(0, 1)
            arrived(along)
            pass_on(across + core * (along - across), along + core * (across - along)).start()

    for d in range(1, n):
        send_tok(d).start()
    gather_first(1)
    for c in load_w:
        c.start()

    for h in range(4):
        k1b[h] = ek[pl.ds(h, 128, stride=4), :].astype(BF16)
        tot[h] = jnp.broadcast_to(jnp.exp(tot1[:, h : h + 1]), (128, 128))

    def recall(t, _):
        load_s(t).wait()
        rows = pl.ds(pl.multiple_of(16 * t, 16), 16)
        for h in range(4):
            wide = jnp.concatenate([state[4 * t + q, h].astype(BF16) for q in range(4)], axis=1)
            r1[h, rows, :] = quad_rows(mm(k1b[h, rows, :], wide), 16)
        return 0

    lax.fori_loop(0, 8, recall, 0, unroll=2)
    gather_first(0)

    for h in range(4):
        b = rate1[:, h : h + 1]
        c_col = cum1[:, h : h + 1]
        kb = k1b[h]
        a = b * ratios(c_col, as_row(c_col, eye), strict) * mm_nt(kb, kb)
        rhs = b * (ev[pl.ds(h, 128, stride=4), :] - jnp.exp(c_col) * r1[h])
        u = rhs + mm(nilpotent(a).astype(BF16), rhs.astype(BF16))
        u1[h] = u * jnp.exp(tot1[:, h : h + 1] - c_col)

    own = lax.broadcasted_iota(jnp.int32, (16, 128), 0) // 4

    def fold(t, _):
        rows = pl.ds(pl.multiple_of(16 * t, 16), 16)
        for h in range(4):
            u = u1[h, rows, :]
            wide = jnp.concatenate([jnp.where(own == q, u, 0.0) for q in range(4)], axis=1).astype(BF16)
            step = lax.dot_general(k1b[h, rows, :], wide, TN, preferred_element_type=F32)
            for q in range(4):
                kept = state[4 * t + q, h] * tot[h, pl.ds(16 * t + 4 * q, 1), :]
                new = kept + step[:, 128 * q : 128 * q + 128]
                state[4 * t + q, h] = new
                state_b[h, t, :, 128 * q : 128 * q + 128] = new.astype(BF16)
        return 0

    lax.fori_loop(0, 8, fold, 0, unroll=2)

    def collect(g):
        group = lax.rem(me // 4 + g, n // 4)
        count = 4 if g else 3
        rows = tok.at[pl.ds(0, 64 * count), :]
        to_peer(rows, rows, tsend, trecv.at[group], me).wait_recv()
        share(g).start()

    def project(g):
        group = lax.rem(me // 4 + g, n // 4)
        share(g).wait_recv()
        pieces = []
        square = jnp.zeros((128, 128), F32)
        for i in range(4):
            wide = x[pl.ds(4 * group + i, 1)][0].astype(F32)
            square = square + wide * wide
            pieces.append((wide * pre_gain[pl.ds(4 * group + i, 1), :]).astype(BF16))
        scaled = jnp.concatenate(pieces, axis=1)
        cols = pl.ds(pl.multiple_of(group * 512, 512), 512)
        beta = mm_nt(scaled, beta_t[:, cols])
        decay = mm_nt(scaled, decay_t[:, cols])
        ssq[...] = square if g == 0 else ssq[...] + square
        scal[0] = beta if g == 0 else scal[0] + beta
        scal[1] = decay if g == 0 else scal[1] + decay
        for i in range(4):
            out = mm(scaled, w[i, cols, :])
            proj[i] = out if g == 0 else proj[i] + out

    groups = n // 4
    for g in range(groups):
        collect(g)
        if g == min(1, groups - 1):
            for c in load_w:
                c.wait()
        if g > 1:
            project(g - 2)
    for g in range(max(groups - 2, 0), groups):
        project(g)
    inverse = lax.rsqrt(jnp.sum(ssq[...], axis=1, keepdims=True) / width + 1e-06)
    beta_raw = scal[0] * inverse
    decay_raw = scal[1] * inverse
    rates8 = 1.0 / (1.0 + jnp.exp(-beta_raw))
    soft8 = jnp.maximum(decay_raw, 0.0) + jnp.log1p(jnp.exp(-jnp.abs(decay_raw)))
    for h in range(4):
        lanes = slice(128 * h, 128 * h + 128)
        q2b[h] = (unit(silu(proj[0, :, lanes] * inverse)) * 128 ** (-0.5)).astype(BF16)
        k2b[h] = unit(silu(proj[1, :, lanes] * inverse)).astype(BF16)
        v2[h] = silu(proj[2, :, lanes] * inverse)
        gates[h] = silu(proj[3, :, lanes] * inverse) * head_gain[...]

    def recall_new(t, _):
        rows = pl.ds(pl.multiple_of(16 * t, 16), 16)
        for h in range(4):
            both = jnp.concatenate([k2b[h, rows, :], q2b[h, rows, :]], axis=0)
            out = quad_rows(mm(both, state_b[h, t]), 32)
            r1[h, rows, :] = out[:16]
            rq[h, rows, :] = out[16:]
        return 0

    gather_second()
    lax.fori_loop(0, 8, recall_new, 0, unroll=2)

    def to_pair(h):
        two = pl.ds(2 * h, 2)
        return to_peer(att.at[0, two], att.at[1, two], asend, arecv, pair)

    upper = core > 0
    for h in range(4):
        b = jnp.where(upper, rates8[:, h + 4 : h + 5], rates8[:, h : h + 1])
        g = jnp.where(upper, soft8[:, h + 4 : h + 5], soft8[:, h : h + 1])
        g = -jnp.exp(decay_log[:, h : h + 1]) * g
        c_col = jnp.sum(jnp.where(incl, as_row(g, eye), 0.0), axis=1, keepdims=True)
        ratio = ratios(c_col, as_row(c_col, eye), incl)
        kb = k2b[h]
        cross = mm_nt(jnp.concatenate([kb, q2b[h]], axis=0), kb)
        a = jnp.where(strict, b * ratio * cross[:128], 0.0)
        seen = ratio * cross[128:]
        seen = seen + mm(seen.astype(BF16), nilpotent(a).astype(BF16))
        grown = jnp.exp(c_col)
        rhs = b * (v2[h] - grown * r1[h])
        reads = grown * rq[h] + mm(seen.astype(BF16), rhs.astype(BF16))
        normed = reads * lax.rsqrt(jnp.mean(reads * reads, axis=-1, keepdims=True) + 1e-06)
        att[0, h] = (normed * gates[h]).astype(BF16)
        if h % 2:
            to_pair(h // 2).start()

    def swap(slot, blocks):
        return pltpu.make_async_remote_copy(
            src_ref=psend.at[slot, blocks], dst_ref=precv.at[slot, blocks], send_sem=xsend, recv_sem=xrecv.at[slot],
            device_id={"kv": me, "tp": 1 - core}, device_id_type=MESH,
        )

    many = n // 4

    def multiply(slot, side):
        attended = jnp.concatenate([att[slot, h] for h in range(4)], axis=1)
        some = jnp.concatenate([wt[pl.ds(place(dz, side), 1)][0] for dz in [0] + far], axis=0)
        out = mm_nt(some, attended).reshape(many, 128, 128)
        blocks = pl.ds(side * many, many)
        part[slot, blocks] = out
        psend[slot, blocks] = out.astype(BF16)
        swap(slot, blocks).start()

    multiply(0, 0)
    for dz in far:
        arrived(place(dz, 1))
    multiply(0, 1)
    to_peer(att.at[0], att.at[1], asend, arecv, pair).wait()
    multiply(1, 0)
    multiply(1, 1)

    def send_sums(d):
        return to_peer(sums.at[me], sums.at[me], ssend, srecv, lax.rem(me + d, n))

    totals = []
    for slot, target in enumerate((me, pair)):
        swap(slot, pl.ds(0, n // 2)).wait_recv()
        squares = jnp.zeros((128, 128), F32)
        for i in range(n // 2):
            both = part[slot, i] + precv[slot, i].astype(F32)
            squares = squares + both * both
        totals.append(jnp.sum(squares, axis=0, keepdims=True))
        if slot:
            first = lax.broadcasted_iota(jnp.int32, (2, 128), 0) == 0
            sums[pl.ds(me, 1)] = jnp.where(first, totals[0], totals[1])[None]
            for d in range(1, n):
                send_sums(d).start()
        for i in range(n // 2):
            both = part[slot, i, half, :] + precv[slot, i, half, :].astype(F32)
            msend[slot, i] = both.astype(BF16)
        mixed_in[pl.ds(target, 1)] = msend[slot, 0][None]
        for i, (dz, side) in enumerate([(dz, side) for side in range(2) for dz in [0] + far]):
            if i:
                to_peer(msend.at[slot, i], mixed_in.at[target], osend, orecv, place(dz, side)).start()
    others = pl.ds(0, n - 2)
    to_peer(mixed_in.at[others], mixed_in.at[others], osend, orecv, me).wait()
    others = pl.ds(0, n - 1)
    to_peer(sums.at[others], sums.at[others], ssend, srecv, me).wait()
    rows = tok.at[pl.ds(0, 64 * (n - 1)), :]
    to_peer(rows, rows, tsend, tsend, me).wait_send()
    mine = x.at[:, half, :]
    to_peer(mine, mine, fsend, fsend, me).wait_send()
    others = pl.ds(0, 1 + 2 * len(far))
    to_peer(wt.at[others], wt.at[others], gsend, gsend, me).wait_send()
    for slot in range(2):
        swap(slot, pl.ds(0, n // 2)).wait_send()


def last_kernel(n, state, mixed_in, sums, post_gain, committed, mixed, rows_out, sem, mixed_sem):
    copies = []
    for t in range(8):
        some = pl.ds(4 * t, 4)
        copies.append(pltpu.make_async_copy(state.at[some], committed.at[some], sem.at[t]))
        copies[t].start()
    i = lax.broadcasted_iota(jnp.int32, (64, 64), 0)
    j = lax.broadcasted_iota(jnp.int32, (64, 64), 1)
    gain = jnp.sum(jnp.where(i == j, post_gain[...], 0.0), axis=1, keepdims=True)
    for k in range(n):
        total = sums[k, 0:1, :] + sums[k + 1 - 2 * (k % 2), 1:2, :]
        factor = lax.rsqrt(total / (n * 128) + 1e-06)
        rows_out[:, 128 * k : 128 * k + 128] = (mixed_in[k].astype(F32) * factor * gain).astype(BF16)
    write_mixed = pltpu.make_async_copy(rows_out, mixed, mixed_sem)
    write_mixed.start()
    for c in copies:
        c.wait()
    write_mixed.wait()


def local(
    n,
    tokens, pre_gain, query_weight, key_weight, value_weight, gate_weight, beta_weight, decay_weight, decay_log,
    head_gain, out_weight, post_gain, saved_state, earlier_keys, earlier_values, earlier_rates, earlier_decays, accepted,
):
    any_spec = pl.BlockSpec(memory_space=pl.ANY)
    vmem = pl.BlockSpec(memory_space=VM)
    dma = pltpu.SemaphoreType.DMA
    heads = (4, 128, 128)
    state, mixed_in, sums = pl.pallas_call(
        functools.partial(main_kernel, n),
        out_shape=(VM(saved_state.shape, F32), VM((n, 64, 128), BF16), VM((n, 2, 128), F32)),
        in_specs=[any_spec] * 17,
        out_specs=(vmem,) * 3,
        scratch_shapes=[
            VM((512, 128), BF16),
            VM((512, 128), BF16),
            VM((4, 4, 32), F32),
            VM((4, 4, 32), F32),
            VM((1, 32), jnp.int32),
            VM((n, 128), F32),
            VM((8, n * 128), BF16),
            VM((8, n * 128), BF16),
            VM((1, 4), F32),
            VM((1, 128), F32),
            VM((n * 128, 128), BF16),
            VM((n, 128, 128), BF16),
            VM((4, n * 128, 512), BF16),
            VM((512, 128), BF16),
            VM((n, 128, 512), BF16),
            VM((4, 8, 128, 512), BF16),
            VM((512, 128), F32),
            VM((512, 128), F32),
            VM(heads, BF16),
            VM(heads, F32),
            VM(heads, F32),
            VM(heads, F32),
            VM(heads, F32),
            VM(heads, BF16),
            VM(heads, BF16),
            VM(heads, F32),
            VM(heads, F32),
            VM((4, 128, 512), F32),
            VM((2, 128, 8), F32),
            VM((128, 128), F32),
            VM((2, 4, 128, 128), BF16),
            VM((2, n // 2, 128, 128), F32),
            VM((2, n // 2, 128, 128), BF16),
            VM((2, n // 2, 128, 128), BF16),
            VM((2, n // 2, 64, 128), BF16),
            dma, dma, dma((8,)), dma((4,)), dma((10,)),
            dma, dma((n // 4,)), dma, dma((n,)), dma, dma((2,)), dma, dma, dma, dma((n // 4,)), dma, dma, dma, dma,
        ],
        compiler_params=pltpu.CompilerParams(collective_id=0, has_side_effects=True, vmem_limit_bytes=48 << 20),
        name="delta_step",
    )(
        tokens, out_weight, saved_state, query_weight, key_weight, value_weight, gate_weight,
        earlier_keys.reshape(512, 128), earlier_values.reshape(512, 128), earlier_rates.transpose(1, 2, 0),
        earlier_decays.transpose(1, 2, 0), accepted.reshape(1, 32), pre_gain.reshape(n, 128), beta_weight.T,
        decay_weight.T, decay_log.reshape(1, 4), head_gain.reshape(1, 128),
    )
    committed, mixed = pl.pallas_call(
        functools.partial(last_kernel, n),
        out_shape=(jax.ShapeDtypeStruct(saved_state.shape, F32), jax.ShapeDtypeStruct((64, n * 128), BF16)),
        in_specs=[vmem] * 4,
        out_specs=(any_spec, any_spec),
        scratch_shapes=[VM((64, n * 128), BF16), dma((8,)), dma],
        compiler_params=pltpu.CompilerParams(vmem_limit_bytes=16 << 20),
        name="write_out",
    )(state, mixed_in, sums, post_gain.reshape(1, 64))
    return mixed.T, committed


def solution(mesh):
    placed = (
        P("dp", "kv"), P(), P(None, "tp"), P(None, "tp"), P(None, "tp"), P(None, "tp"), P(), P(), P("tp"), P(),
        P("tp", "kv"), P(("kv", "tp")), P(("dp", "kv"), "tp", None, None), P(("dp", "kv"), None, "tp", None),
        P(("dp", "kv"), None, "tp", None), P(("dp", "kv"), None, "tp"), P(("dp", "kv"), None, "tp"), P(("dp", "kv")),
    )
    return jax.shard_map(
        functools.partial(local, mesh.shape["kv"]),
        mesh=mesh,
        in_specs=placed,
        out_specs=(P("dp", ("kv", "tp")), P(("dp", "kv"), "tp", None, None)),
        check_vma=False,
    )
```

```python
import functools

import jax
import jax.numpy as jnp
from jax import lax
from jax.experimental import pallas as pl
from jax.experimental.pallas import tpu as pltpu
from jax.sharding import PartitionSpec as P

MESH = pl.DeviceIdType.MESH
F32 = jnp.float32
BF16 = jnp.bfloat16
HIGH = lax.Precision.HIGHEST
VM = pltpu.VMEM
NT = (((1,), (1,)), ((), ()))
TN = (((0,), (0,)), ((), ()))


def mm(a, b):
    return jnp.dot(a, b, preferred_element_type=F32)


def mm_nt(a, b):
    return lax.dot_general(a, b, NT, preferred_element_type=F32)


def silu(v):
    return v / (1.0 + jnp.exp(-v))


def unit(v):
    return v * lax.rsqrt(jnp.sum(v * v, axis=-1, keepdims=True) + 1e-06)


def quad_rows(wide, rows):
    own = lax.broadcasted_iota(jnp.int32, (rows, 128), 0) % 16 // 4
    out = wide[:, 0:128]
    for q in range(1, 4):
        out = jnp.where(own == q, wide[:, 128 * q : 128 * q + 128], out)
    return out


def masks():
    r = lax.broadcasted_iota(jnp.int32, (128, 128), 0)
    c = lax.broadcasted_iota(jnp.int32, (128, 128), 1)
    same = r // 4 == c // 4
    return r == c, same & (c < r), same & (c <= r)


def as_row(col, eye):
    return jnp.sum(jnp.where(eye, col, 0.0), axis=0, keepdims=True)


def ratios(c_col, c_row, keep):
    return jnp.where(keep, jnp.exp(jnp.where(keep, c_col - c_row, 0.0)), 0.0)


def nilpotent(a):
    ab = a.astype(BF16)
    square = mm(ab, ab)
    return square - a - mm(ab, square.astype(BF16))


def main_kernel(
    n,
    tokens, out_w, saved, wq, wk, wv, wg,
    ekeys_in, evals_in, erates_in, edecays_in, accepted_in, pre_gain_in, beta_in, decay_in, decay_log_in, head_gain_in,
    state, mixed_in, sums,
    ekeys, evals, erates, edecays, accepted, pre_gain, beta_t, decay_t, decay_log, head_gain,
    tok, x, w, ow, wt, state_b, ek, ev, k1b, u1, tot, r1, rq, k2b, q2b, v2, gates, proj, scal, ssq, att,
    part, psend, precv, msend,
    tok_sem, ow_sem, s_sem, w_sem, small_sem, tsend, trecv, gsend, grecv, xsend, xrecv, osend, orecv, fsend, frecv,
    asend, arecv, ssend, srecv,
):
    me = lax.axis_index("kv")
    core = lax.axis_index("tp")
    width = n * 128

    barrier = pltpu.get_barrier_semaphore()
    for d in range(1, n):
        pl.semaphore_signal(barrier, inc=1, device_id={"kv": lax.rem(me + d, n), "tp": core}, device_id_type=MESH)
    pl.semaphore_signal(barrier, inc=1, device_id={"kv": me, "tp": 1 - core}, device_id_type=MESH)

    load_tok = pltpu.make_async_copy(tokens, tok, tok_sem)
    load_ow = pltpu.make_async_copy(out_w, ow, ow_sem)
    load_ow.start()
    load_tok.start()
    small = (
        (ekeys_in, ekeys), (evals_in, evals), (erates_in, erates), (edecays_in, edecays), (accepted_in, accepted),
        (pre_gain_in, pre_gain), (beta_in, beta_t), (decay_in, decay_t), (decay_log_in, decay_log), (head_gain_in, head_gain),
    )
    load_small = [pltpu.make_async_copy(src, dst, small_sem.at[i]) for i, (src, dst) in enumerate(small)]
    for c in load_small:
        c.start()

    def load_s(t):
        some = pl.ds(4 * t, 4)
        return pltpu.make_async_copy(saved.at[some], state.at[some], s_sem.at[t])

    load_w = [pltpu.make_async_copy(src, w.at[i], w_sem.at[i]) for i, src in enumerate((wq, wk, wv, wg))]

    eye, strict, incl = masks()
    load_ow.wait()
    load_tok.wait()
    for c in load_small:
        c.wait()
    for t in range(8):
        load_s(t).start()
    wt[pl.ds(me, 1)] = mm_nt(jnp.where(eye, 1.0, 0.0).astype(BF16), ow[...]).astype(BF16)[None]
    half = pl.ds(pl.multiple_of(core * 64, 64), 64)
    x[pl.ds(me, 1), half, :] = tok[pl.ds(pl.multiple_of(me * 128 + core * 64, 64), 64), :][None]

    keys = unit(ekeys[...].astype(F32))
    ek[...] = keys
    ev[...] = evals[...].astype(F32)
    count = accepted[...]
    total = jnp.zeros((4, 32), F32)
    rate_p, cum_p = [], []
    for p in range(4):
        live = jnp.where(p < count, 1.0, 0.0)
        total = total + edecays[p] * live
        rate_p.append(erates[p] * live)
        cum_p.append(total)
    row = lax.broadcasted_iota(jnp.int32, (128, 32), 0)
    seq = lax.broadcasted_iota(jnp.int32, (128, 32), 1)

    def expand(pieces):
        out = jnp.zeros((128, 4), F32)
        for p in range(4):
            pick = jnp.where(row == 4 * seq + p, 1.0, 0.0)
            out = out + lax.dot_general(pick, pieces[p], NT, precision=HIGH, preferred_element_type=F32)
        return out

    rate1 = expand(rate_p)
    cum1 = expand(cum_p)
    tot1 = expand([total] * 4)
    pl.semaphore_wait(barrier, n)

    def to_peer(src, dst, ssem, rsem, peer):
        return pltpu.make_async_remote_copy(
            src_ref=src, dst_ref=dst, send_sem=ssem, recv_sem=rsem,
            device_id={"kv": peer, "tp": core}, device_id_type=MESH,
        )

    def send_tok(d):
        peer = lax.rem(me + d, n)
        rows = pl.ds(pl.multiple_of(peer * 128 + core * 64, 64), 64)
        return to_peer(tok.at[rows, :], x.at[me, half, :], tsend, trecv.at[me // 4], peer)

    def share(g):
        some = x.at[pl.ds(4 * lax.rem(me // 4 + g, n // 4), 4), half, :]
        return pltpu.make_async_remote_copy(
            src_ref=some, dst_ref=some, send_sem=fsend, recv_sem=frecv.at[g],
            device_id={"kv": me, "tp": 1 - core}, device_id_type=MESH,
        )

    at_z, at_y = me // 4, lax.rem(me, 4)
    pair = me + 1 - 2 * lax.rem(at_y, 2)

    def place(dz, side):
        return lax.rem(at_z + dz, n // 4) * 4 + at_y + side * (3 - 2 * at_y)

    def pass_on(block, peer):
        return to_peer(wt.at[block], wt.at[block], gsend, grecv.at[block], peer)

    def arrived(block):
        pass_on(block, me).wait_recv()

    far = [dz for dz in (2, 1, 3) if dz < n // 4]

    def gather_first(along):
        @pl.when(core == along)
        def _():
            for dz in far:
                pass_on(me, place(dz, 0)).start()

        @pl.when(core != along)
        def _():
            pass_on(me, place(0, 1)).start()

    def gather_second():
        arrived(place(0, 1))
        for dz in far:
            along, across = place(dz, 0), place(0, 1)
            arrived(along)
            pass_on(across + core * (along - across), along + core * (across - along)).start()

    for d in range(1, n):
        send_tok(d).start()
    gather_first(1)
    for c in load_w:
        c.start()

    for h in range(4):
        k1b[h] = ek[pl.ds(h, 128, stride=4), :].astype(BF16)
        tot[h] = jnp.broadcast_to(jnp.exp(tot1[:, h : h + 1]), (128, 128))

    def recall(t, _):
        load_s(t).wait()
        rows = pl.ds(pl.multiple_of(16 * t, 16), 16)
        for h in range(4):
            wide = jnp.concatenate([state[4 * t + q, h].astype(BF16) for q in range(4)], axis=1)
            r1[h, rows, :] = quad_rows(mm(k1b[h, rows, :], wide), 16)
        return 0

    lax.fori_loop(0, 8, recall, 0, unroll=2)
    gather_first(0)

    for h in range(4):
        b = rate1[:, h : h + 1]
        c_col = cum1[:, h : h + 1]
        kb = k1b[h]
        a = b * ratios(c_col, as_row(c_col, eye), strict) * mm_nt(kb, kb)
        rhs = b * (ev[pl.ds(h, 128, stride=4), :] - jnp.exp(c_col) * r1[h])
        u = rhs + mm(nilpotent(a).astype(BF16), rhs.astype(BF16))
        u1[h] = u * jnp.exp(tot1[:, h : h + 1] - c_col)

    own = lax.broadcasted_iota(jnp.int32, (16, 128), 0) // 4

    def fold(t, _):
        rows = pl.ds(pl.multiple_of(16 * t, 16), 16)
        for h in range(4):
            u = u1[h, rows, :]
            wide = jnp.concatenate([jnp.where(own == q, u, 0.0) for q in range(4)], axis=1).astype(BF16)
            step = lax.dot_general(k1b[h, rows, :], wide, TN, preferred_element_type=F32)
            for q in range(4):
                kept = state[4 * t + q, h] * tot[h, pl.ds(16 * t + 4 * q, 1), :]
                new = kept + step[:, 128 * q : 128 * q + 128]
                state[4 * t + q, h] = new
                state_b[h, t, :, 128 * q : 128 * q + 128] = new.astype(BF16)
        return 0

    lax.fori_loop(0, 8, fold, 0, unroll=2)

    def collect(g):
        group = lax.rem(me // 4 + g, n // 4)
        count = 4 if g else 3
        rows = tok.at[pl.ds(0, 64 * count), :]
        to_peer(rows, rows, tsend, trecv.at[group], me).wait_recv()
        share(g).start()

    def project(g):
        group = lax.rem(me // 4 + g, n // 4)
        share(g).wait_recv()
        pieces = []
        square = jnp.zeros((128, 128), F32)
        for i in range(4):
            wide = x[pl.ds(4 * group + i, 1)][0].astype(F32)
            square = square + wide * wide
            pieces.append((wide * pre_gain[pl.ds(4 * group + i, 1), :]).astype(BF16))
        scaled = jnp.concatenate(pieces, axis=1)
        cols = pl.ds(pl.multiple_of(group * 512, 512), 512)
        beta = mm_nt(scaled, beta_t[:, cols])
        decay = mm_nt(scaled, decay_t[:, cols])
        ssq[...] = square if g == 0 else ssq[...] + square
        scal[0] = beta if g == 0 else scal[0] + beta
        scal[1] = decay if g == 0 else scal[1] + decay
        for i in range(4):
            out = mm(scaled, w[i, cols, :])
            proj[i] = out if g == 0 else proj[i] + out

    groups = n // 4
    near = [g for g in (0, 1, 3, 2) if g < groups]
    for g in range(groups):
        collect(near[g])
        if g == min(1, groups - 1):
            for c in load_w:
                c.wait()
        if g > 1:
            project(near[g - 2])
    for g in range(max(groups - 2, 0), groups):
        project(near[g])
    inverse = lax.rsqrt(jnp.sum(ssq[...], axis=1, keepdims=True) / width + 1e-06)
    beta_raw = scal[0] * inverse
    decay_raw = scal[1] * inverse
    rates8 = 1.0 / (1.0 + jnp.exp(-beta_raw))
    soft8 = jnp.maximum(decay_raw, 0.0) + jnp.log1p(jnp.exp(-jnp.abs(decay_raw)))
    for h in range(4):
        lanes = slice(128 * h, 128 * h + 128)
        q2b[h] = (unit(silu(proj[0, :, lanes] * inverse)) * 128 ** (-0.5)).astype(BF16)
        k2b[h] = unit(silu(proj[1, :, lanes] * inverse)).astype(BF16)
        v2[h] = silu(proj[2, :, lanes] * inverse)
        gates[h] = silu(proj[3, :, lanes] * inverse) * head_gain[...]

    def recall_new(t, _):
        rows = pl.ds(pl.multiple_of(16 * t, 16), 16)
        for h in range(4):
            both = jnp.concatenate([k2b[h, rows, :], q2b[h, rows, :]], axis=0)
            out = quad_rows(mm(both, state_b[h, t]), 32)
            r1[h, rows, :] = out[:16]
            rq[h, rows, :] = out[16:]
        return 0

    gather_second()
    lax.fori_loop(0, 8, recall_new, 0, unroll=2)

    def to_pair(h):
        some = pl.ds(0, 3) if h == 2 else pl.ds(3, 1)
        return to_peer(att.at[0, some], att.at[1, some], asend, arecv, pair)

    upper = core > 0
    for h in range(4):
        b = jnp.where(upper, rates8[:, h + 4 : h + 5], rates8[:, h : h + 1])
        g = jnp.where(upper, soft8[:, h + 4 : h + 5], soft8[:, h : h + 1])
        g = -jnp.exp(decay_log[:, h : h + 1]) * g
        c_col = jnp.sum(jnp.where(incl, as_row(g, eye), 0.0), axis=1, keepdims=True)
        ratio = ratios(c_col, as_row(c_col, eye), incl)
        kb = k2b[h]
        cross = mm_nt(jnp.concatenate([kb, q2b[h]], axis=0), kb)
        a = jnp.where(strict, b * ratio * cross[:128], 0.0)
        seen = ratio * cross[128:]
        seen = seen + mm(seen.astype(BF16), nilpotent(a).astype(BF16))
        grown = jnp.exp(c_col)
        rhs = b * (v2[h] - grown * r1[h])
        reads = grown * rq[h] + mm(seen.astype(BF16), rhs.astype(BF16))
        normed = reads * lax.rsqrt(jnp.mean(reads * reads, axis=-1, keepdims=True) + 1e-06)
        att[0, h] = (normed * gates[h]).astype(BF16)
        if h > 1:
            to_pair(h).start()

    def swap(slot, blocks):
        return pltpu.make_async_remote_copy(
            src_ref=psend.at[slot, blocks], dst_ref=precv.at[slot, blocks], send_sem=xsend, recv_sem=xrecv.at[slot],
            device_id={"kv": me, "tp": 1 - core}, device_id_type=MESH,
        )

    many = n // 4

    def multiply(slot, sides):
        attended = jnp.concatenate([att[slot, h] for h in range(4)], axis=1)
        some = jnp.concatenate([wt[pl.ds(place(dz, side), 1)][0] for side in sides for dz in [0] + far], axis=0)
        out = mm_nt(some, attended).reshape(many * len(sides), 128, 128)
        blocks = pl.ds(sides[0] * many, many * len(sides))
        part[slot, blocks] = out
        psend[slot, blocks] = out.astype(BF16)
        swap(slot, blocks).start()

    multiply(0, (0,))
    for dz in far:
        arrived(place(dz, 1))
    multiply(0, (1,))
    to_peer(att.at[0], att.at[1], asend, arecv, pair).wait()
    multiply(1, (0, 1))

    def send_sums(d):
        return to_peer(sums.at[me], sums.at[me], ssend, srecv, lax.rem(me + d, n))

    totals = []
    for slot, target in enumerate((me, pair)):
        swap(slot, pl.ds(0, n // 2)).wait_recv()
        squares = jnp.zeros((128, 128), F32)
        for i in range(n // 2):
            both = part[slot, i] + precv[slot, i].astype(F32)
            squares = squares + both * both
        totals.append(jnp.sum(squares, axis=0, keepdims=True))
        if slot:
            first = lax.broadcasted_iota(jnp.int32, (2, 128), 0) == 0
            sums[pl.ds(me, 1)] = jnp.where(first, totals[0], totals[1])[None]
            for d in range(1, n):
                send_sums(d).start()
        for i in range(n // 2):
            both = part[slot, i, half, :] + precv[slot, i, half, :].astype(F32)
            msend[slot, i] = both.astype(BF16)
        mixed_in[pl.ds(target, 1)] = msend[slot, 0][None]
        for i, (dz, side) in enumerate([(dz, side) for side in range(2) for dz in [0] + far]):
            if i:
                to_peer(msend.at[slot, i], mixed_in.at[target], osend, orecv, place(dz, side)).start()
    others = pl.ds(0, n - 2)
    to_peer(mixed_in.at[others], mixed_in.at[others], osend, orecv, me).wait()
    others = pl.ds(0, n - 1)
    to_peer(sums.at[others], sums.at[others], ssend, srecv, me).wait()
    rows = tok.at[pl.ds(0, 64 * (n - 1)), :]
    to_peer(rows, rows, tsend, tsend, me).wait_send()
    mine = x.at[:, half, :]
    to_peer(mine, mine, fsend, fsend, me).wait_send()
    others = pl.ds(0, 1 + 2 * len(far))
    to_peer(wt.at[others], wt.at[others], gsend, gsend, me).wait_send()
    for slot in range(2):
        swap(slot, pl.ds(0, n // 2)).wait_send()


def last_kernel(n, state, mixed_in, sums, post_gain, committed, mixed, rows_out, sem, mixed_sem):
    copies = []
    for t in range(8):
        some = pl.ds(4 * t, 4)
        copies.append(pltpu.make_async_copy(state.at[some], committed.at[some], sem.at[t]))
        copies[t].start()
    i = lax.broadcasted_iota(jnp.int32, (64, 64), 0)
    j = lax.broadcasted_iota(jnp.int32, (64, 64), 1)
    gain = jnp.sum(jnp.where(i == j, post_gain[...], 0.0), axis=1, keepdims=True)
    for k in range(n):
        total = sums[k, 0:1, :] + sums[k + 1 - 2 * (k % 2), 1:2, :]
        factor = lax.rsqrt(total / (n * 128) + 1e-06)
        rows_out[:, 128 * k : 128 * k + 128] = (mixed_in[k].astype(F32) * factor * gain).astype(BF16)
    write_mixed = pltpu.make_async_copy(rows_out, mixed, mixed_sem)
    write_mixed.start()
    for c in copies:
        c.wait()
    write_mixed.wait()


def local(
    n,
    tokens, pre_gain, query_weight, key_weight, value_weight, gate_weight, beta_weight, decay_weight, decay_log,
    head_gain, out_weight, post_gain, saved_state, earlier_keys, earlier_values, earlier_rates, earlier_decays, accepted,
):
    any_spec = pl.BlockSpec(memory_space=pl.ANY)
    vmem = pl.BlockSpec(memory_space=VM)
    dma = pltpu.SemaphoreType.DMA
    heads = (4, 128, 128)
    state, mixed_in, sums = pl.pallas_call(
        functools.partial(main_kernel, n),
        out_shape=(VM(saved_state.shape, F32), VM((n, 64, 128), BF16), VM((n, 2, 128), F32)),
        in_specs=[any_spec] * 17,
        out_specs=(vmem,) * 3,
        scratch_shapes=[
            VM((512, 128), BF16),
            VM((512, 128), BF16),
            VM((4, 4, 32), F32),
            VM((4, 4, 32), F32),
            VM((1, 32), jnp.int32),
            VM((n, 128), F32),
            VM((8, n * 128), BF16),
            VM((8, n * 128), BF16),
            VM((1, 4), F32),
            VM((1, 128), F32),
            VM((n * 128, 128), BF16),
            VM((n, 128, 128), BF16),
            VM((4, n * 128, 512), BF16),
            VM((512, 128), BF16),
            VM((n, 128, 512), BF16),
            VM((4, 8, 128, 512), BF16),
            VM((512, 128), F32),
            VM((512, 128), F32),
            VM(heads, BF16),
            VM(heads, F32),
            VM(heads, F32),
            VM(heads, F32),
            VM(heads, F32),
            VM(heads, BF16),
            VM(heads, BF16),
            VM(heads, F32),
            VM(heads, F32),
            VM((4, 128, 512), F32),
            VM((2, 128, 8), F32),
            VM((128, 128), F32),
            VM((2, 4, 128, 128), BF16),
            VM((2, n // 2, 128, 128), F32),
            VM((2, n // 2, 128, 128), BF16),
            VM((2, n // 2, 128, 128), BF16),
            VM((2, n // 2, 64, 128), BF16),
            dma, dma, dma((8,)), dma((4,)), dma((10,)),
            dma, dma((n // 4,)), dma, dma((n,)), dma, dma((2,)), dma, dma, dma, dma((n // 4,)), dma, dma, dma, dma,
        ],
        compiler_params=pltpu.CompilerParams(collective_id=0, has_side_effects=True, vmem_limit_bytes=48 << 20),
        name="delta_step",
    )(
        tokens, out_weight, saved_state, query_weight, key_weight, value_weight, gate_weight,
        earlier_keys.reshape(512, 128), earlier_values.reshape(512, 128), earlier_rates.transpose(1, 2, 0),
        earlier_decays.transpose(1, 2, 0), accepted.reshape(1, 32), pre_gain.reshape(n, 128), beta_weight.T,
        decay_weight.T, decay_log.reshape(1, 4), head_gain.reshape(1, 128),
    )
    committed, mixed = pl.pallas_call(
        functools.partial(last_kernel, n),
        out_shape=(jax.ShapeDtypeStruct(saved_state.shape, F32), jax.ShapeDtypeStruct((64, n * 128), BF16)),
        in_specs=[vmem] * 4,
        out_specs=(any_spec, any_spec),
        scratch_shapes=[VM((64, n * 128), BF16), dma((8,)), dma],
        compiler_params=pltpu.CompilerParams(vmem_limit_bytes=16 << 20),
        name="write_out",
    )(state, mixed_in, sums, post_gain.reshape(1, 64))
    return mixed.T, committed


def solution(mesh):
    placed = (
        P("dp", "kv"), P(), P(None, "tp"), P(None, "tp"), P(None, "tp"), P(None, "tp"), P(), P(), P("tp"), P(),
        P("tp", "kv"), P(("kv", "tp")), P(("dp", "kv"), "tp", None, None), P(("dp", "kv"), None, "tp", None),
        P(("dp", "kv"), None, "tp", None), P(("dp", "kv"), None, "tp"), P(("dp", "kv"), None, "tp"), P(("dp", "kv")),
    )
    return jax.shard_map(
        functools.partial(local, mesh.shape["kv"]),
        mesh=mesh,
        in_specs=placed,
        out_specs=(P("dp", ("kv", "tp")), P(("dp", "kv"), "tp", None, None)),
        check_vma=False,
    )
```
